32 devices in a mesh: ep: 4 (over y, x), tp: 8 (over z, core).
Axes of the slice: x: 2, y: 2, z: 4, core: 2. Of those that a mesh axis runs over, the one named last changes fastest.
Arguments:
- query_preactivation: bfloat16 [8192, 2048], P('ep', 'tp'), may hold values from -6 to 6
- forget_preactivation: bfloat16 [8192, 2048], P('ep', 'tp'), may hold values from -6 to 6
- value_input_rows: bfloat16 [8192, 1024], P('ep', 'tp'), may hold values from -8 to 8
- output_gate_preactivation: bfloat16 [8192, 1024], P('ep', 'tp'), may hold values from -6 to 6
- forget_floor_gap: float32 [2048], P('tp'), may hold values from 0 to 0.2, as said below
- extra_log_forget: float32 [8192, 16], P('ep', 'tp'), may hold values from -2 to 0
- head_output_gain: float32 [1024], P('tp'), may hold values from 0.1 to 1.9
- mixer_output_weight: bfloat16 [1024, 2048], P(None, 'tp'), may hold values from -0.1875 to 0.1875
- second_batch_tokens: bfloat16 [2048, 2048], P('ep'), may hold values from -6 to 6
- feedforward_norm_gain: float32 [2048], replicated, may hold values from 0.1 to 1.9
- chosen_expert_index: int32 [2048, 2], P('ep'), may hold values from 0 to 3, all different within a row; in each aligned block of 64 rows (0 to 63, 64 to 127, ...) at most 40 rows name the same one
- chosen_expert_weight: float32 [2048, 2], P('ep'), may hold values from 0.1 to 1
- expert_gate_weight: bfloat16 [4, 2048, 7168], P('ep', None, 'tp'), may hold values from -0.125 to 0.125
- expert_up_weight: bfloat16 [4, 2048, 7168], P('ep', None, 'tp'), may hold values from -0.125 to 0.125
- expert_down_weight: bfloat16 [4, 7168, 2048], P('ep', 'tp'), may hold values from -0.0625 to 0.0625
Outputs:
- mixer_output_first: bfloat16 [8192, 2048], P('ep', 'tp')
- moe_out: bfloat16 [2048, 2048], P(('ep', 'tp'))
The draws below stay inside these ranges and needn't reach their ends.
Inputs may be any that keep to these rules, and one draw needn't show every extreme that they name: `chosen_expert_index`: each row names 2 different experts. In each aligned block of 64 rows (the rows of one device's share) no expert is named by more than 40 rows, and in every draw some expert is named by exactly 40 rows of some block. `forget_floor_gap`: every entry is positive.
All inputs are finite; a program needn't handle non-finite values.
Results may differ from the reference program's by a relative error of at most 0.019.
Values may be sent and summed in bfloat16 or wider, within the bound.
A program may use at most 128 MiB of HBM per device.

```python
import math
import jax
import jax.numpy as jnp
import numpy as np
from jax import lax

D = 2048
RECURRENT_HEADS = 16
KEY_DIM = 128
VAL_DIM = 64
KW = 2048
VW = 1024
BLOCK_POSITIONS = 64
SEG_A = 2048
TOKENS_A = 8192
TOKENS_B = 2048
SUB_B = 64
EXPERTS = 4
FFE = 7168
FFE_DEV = 896
TOPK = 2
CAP = 40
N_TP = 8


def draw_value_input_rows(key, part):
    noise_key, offset_key = jax.random.split(key)
    noise_part = jnp.clip(jax.random.normal(noise_key, (TOKENS_A, VW), jnp.float32), -6.0, 6.0)
    offsets = jax.random.uniform(offset_key, (1, VW), jnp.float32, -1.0, 1.0)
    return (noise_part + offsets).astype(jnp.bfloat16)


def draw_forget_floor_gap(key, part):
    choose_key, slow_key, fast_key = jax.random.split(key, 3)
    slow_share = 0.5
    chosen = jax.random.uniform(choose_key, (KW,), jnp.float32) < slow_share
    slow_rate = jnp.exp(jax.random.uniform(slow_key, (KW,), jnp.float32, jnp.log(0.05 / TOKENS_A), jnp.log(1.0 / TOKENS_A)))
    fast_rate = jnp.exp(jax.random.uniform(fast_key, (KW,), jnp.float32, jnp.log(0.06), jnp.log(0.2)))
    return jnp.where(chosen, slow_rate, fast_rate)


def draw_extra_log_forget(key, part):
    rate_key, place_key, depth_key = jax.random.split(key, 3)
    segments = TOKENS_A // SEG_A
    rates = jnp.exp(jax.random.uniform(rate_key, (segments, 1, RECURRENT_HEADS), jnp.float32, jnp.log(0.1 / TOKENS_A), jnp.log(0.4 / TOKENS_A)))
    base_log = -jnp.broadcast_to(rates, (segments, SEG_A, RECURRENT_HEADS)).reshape(TOKENS_A, RECURRENT_HEADS)
    places = jax.random.randint(place_key, (2, RECURRENT_HEADS), 0, TOKENS_A)
    depths = jax.random.uniform(depth_key, (2, RECURRENT_HEADS), jnp.float32, jnp.log(0.5), jnp.log(0.8))
    columns = jnp.broadcast_to(jnp.arange(RECURRENT_HEADS, dtype=jnp.int32)[None, :], (2, RECURRENT_HEADS))
    return base_log.at[places, columns].add(depths)


def block_scale(own_key, shape, shards, least, high):
    level, own = 1.0, jax.random.fold_in(own_key, 6)
    for axis_at, shards_of in shards:
        heights = jnp.exp(jax.random.uniform(jax.random.fold_in(own, axis_at), (shards_of,), jnp.float32, least / len(shards), high / len(shards)))
        level = level * jnp.repeat(heights, shape[axis_at] // shards_of).reshape([-1 if axis == axis_at else 1 for axis in range(len(shape))])
    return level


def assign_block(own_key, own, number, rows, count, top, limit, lean):
    ranking = jax.random.permutation(own_key, count)
    crowded, usual = portions_of(count, rows * top, limit, lean, True), portions_of(count, rows * top, limit, lean, False)
    places = jnp.arange(count)

    def named(lengths, turn):
        used = int((lengths > 0).sum())
        fixed = max(1, used // 4)
        shifted = fixed + (places - fixed + turn * (used - fixed)) % max(1, count - fixed)
        return jnp.zeros((count,), jnp.int32).at[ranking[jnp.where(places < fixed, places, shifted)]].set(jnp.asarray(lengths, jnp.int32))

    lengths = jnp.where(number % 4 == 0, named(crowded, number // 4), named(usual, number - number // 4 - 1))
    mixed = jax.random.permutation(jax.random.fold_in(own, 3), count)
    giver, receiver = mixed[0:count // 2 * 2:2], mixed[1:count // 2 * 2:2]
    room = jnp.minimum(lengths[giver] - 1, limit - lengths[receiver]) // 2
    room = jnp.where((giver == ranking[0]) | (receiver == ranking[0]) | (lengths[receiver] == 0), 0, jnp.maximum(room, 0))
    shifted = jax.random.randint(jax.random.fold_in(own, 4), (count // 2,), 0, 1 << 20) % (room + 1)
    lengths = lengths.at[giver].add(-shifted).at[receiver].add(shifted)
    labels = jnp.searchsorted(jnp.cumsum(lengths), jnp.arange(rows * top), side="right").astype(jnp.int32)
    listing = labels.reshape(top, rows).T
    listing = listing[jax.random.permutation(jax.random.fold_in(own, 1), rows)]
    turn = jax.random.randint(jax.random.fold_in(own, 2), (rows, 1), 0, top)
    return jnp.take_along_axis(listing, (jnp.arange(top)[None, :] + turn) % top, axis=1)


def portions_of(amount, total, reach, skew, full):
    portions = [(1 << 20) // math.isqrt(grade ** skew) + 1 for grade in range(1, amount + 1)]
    largest = reach if full else min(reach, max(-(-total // amount), total * portions[0] // sum(portions)))
    least = 1 if total - largest >= amount - 1 else 0
    counts, spare = [largest] + [least] * (amount - 1), total - largest - least * (amount - 1)
    while spare > 0:
        candidates = [i for i in range(1, amount) if counts[i] < largest] or [i for i in range(1, amount) if counts[i] < reach]
        pool, left = sum([portions[i] for i in candidates]), spare
        for i in candidates:
            more = min(reach - counts[i], max(1, left * portions[i] // pool), spare)
            counts[i] = counts[i] + more
            spare = spare - more
    return np.array(counts)


def scatter_about(own_key, dims, deviation, bound, cuts=(), kind=jnp.bfloat16):
    array = deviation * jax.random.normal(own_key, dims, jnp.float32)
    if cuts:
        array = array * block_scale(own_key, dims, cuts, -0.22, 0.18)
    return jnp.clip(array, -bound, bound).astype(kind)


def setup_inputs(seed: int = 0) -> dict:
    key_of = jax.random.split(jax.random.key(seed), 16)
    query_preactivation = scatter_about(key_of[0], (TOKENS_A, KW), 1.0, 6.0, ((0, 4), (1, 8)))
    forget_preactivation = scatter_about(key_of[1], (TOKENS_A, KW), 1.0, 6.0, ((0, 4), (1, 8)))
    value_input_rows = draw_value_input_rows(jax.random.fold_in(key_of[15], 71), 0)
    output_gate_preactivation = scatter_about(key_of[3], (TOKENS_A, VW), 1.0, 6.0, ((0, 4), (1, 8)))
    forget_floor_gap = draw_forget_floor_gap(jax.random.fold_in(key_of[15], 71), 0)
    extra_log_forget = draw_extra_log_forget(jax.random.fold_in(key_of[15], 71), 0)
    head_output_gain = jnp.clip(1.0 + 0.18 * jax.random.normal(key_of[6], (VW,), jnp.float32), 0.1, 1.9)
    mixer_output_weight = scatter_about(key_of[7], (VW, D), VW ** -0.5, 0.1875, ((1, 8),))
    second_batch_tokens = scatter_about(key_of[8], (TOKENS_B, D), 1.0, 6.0, ((0, 4),))
    feedforward_norm_gain = jnp.clip(1.0 + 0.18 * jax.random.normal(key_of[9], (D,), jnp.float32), 0.1, 1.9)
    chosen_expert_index_keys = jax.random.split(jax.random.fold_in(key_of[10], 1), TOKENS_B // SUB_B)
    chosen_expert_index_turns = jax.random.permutation(jax.random.fold_in(key_of[10], 3), TOKENS_B // SUB_B)
    chosen_expert_index = jax.vmap(lambda own, number: assign_block(jax.random.fold_in(key_of[10], 2), own, number, SUB_B, EXPERTS, TOPK, CAP, 1))(chosen_expert_index_keys, chosen_expert_index_turns).reshape((TOKENS_B, TOPK))
    chosen_expert_weight = jnp.clip(0.1 + 0.9 * jax.random.uniform(key_of[11], (TOKENS_B, TOPK), jnp.float32) ** block_scale(key_of[11], (TOKENS_B, TOPK), ((0, 4),), -0.2, 0.2), 0.1, 1.0)
    expert_gate_weight = scatter_about(key_of[12], (EXPERTS, D, FFE), D ** -0.5, 0.125, ((0, 4), (2, 8)))
    expert_up_weight = scatter_about(key_of[13], (EXPERTS, D, FFE), D ** -0.5, 0.125, ((0, 4), (2, 8)))
    expert_down_weight = scatter_about(key_of[14], (EXPERTS, FFE, D), FFE ** -0.5, 0.0625, ((0, 4), (1, 8)))
    return {"query_preactivation": query_preactivation, "forget_preactivation": forget_preactivation, "value_input_rows": value_input_rows, "output_gate_preactivation": output_gate_preactivation, "forget_floor_gap": forget_floor_gap, "extra_log_forget": extra_log_forget, "head_output_gain": head_output_gain, "mixer_output_weight": mixer_output_weight, "second_batch_tokens": second_batch_tokens, "feedforward_norm_gain": feedforward_norm_gain, "chosen_expert_index": chosen_expert_index, "chosen_expert_weight": chosen_expert_weight, "expert_gate_weight": expert_gate_weight, "expert_up_weight": expert_up_weight, "expert_down_weight": expert_down_weight}


highest_accuracy = lax.Precision.HIGHEST
epsilon = 1e-06

def slot_positions(blocks):
    flattened = blocks.reshape(blocks.shape[0], -1)
    onehot = (flattened[..., None] == jnp.arange(EXPERTS, dtype=jnp.int32)).astype(jnp.int32)
    earlier = jnp.cumsum(onehot, axis=1) - onehot
    return lax.optimization_barrier(jnp.sum(earlier * onehot, axis=-1)).reshape(blocks.shape)

def mixer_portion(query_preactivation, forget_preactivation, value_input_rows, output_gate_preactivation, forget_floor_gap, extra_log_forget, head_output_gain, mixer_output_weight):
    length = query_preactivation.shape[0]
    block_count = length // BLOCK_POSITIONS
    shape_key = (block_count, BLOCK_POSITIONS, RECURRENT_HEADS, KEY_DIM)
    queries = jax.nn.silu(query_preactivation.astype(jnp.float32)).reshape(shape_key)
    key_decay_rates = forget_floor_gap.reshape(RECURRENT_HEADS, KEY_DIM) * jax.nn.sigmoid(-forget_preactivation.astype(jnp.float32)).reshape(shape_key)
    forget_log_factor = jnp.log(1.0 - key_decay_rates) + extra_log_forget.reshape(block_count, BLOCK_POSITIONS, RECURRENT_HEADS)[..., None]
    values = value_input_rows.astype(jnp.float32).reshape(block_count, BLOCK_POSITIONS, RECURRENT_HEADS, VAL_DIM)
    causal_mask = jnp.arange(BLOCK_POSITIONS)[:, None] >= jnp.arange(BLOCK_POSITIONS)[None, :]

    def advance(recurrent_state_matrix, inputs):
        query_block_rows, block_key, value_block_rows, block_log = inputs
        cumulative_log = jnp.cumsum(block_log, axis=0)
        block_final_row = cumulative_log[-1]
        query_scaled = query_block_rows * jnp.exp(cumulative_log - block_final_row)
        scaled_key_rows = block_key * jnp.exp(block_final_row - cumulative_log)
        scores = jnp.einsum('thk,shk->hts', query_scaled, scaled_key_rows, precision=highest_accuracy)
        scores = jnp.where(causal_mask, scores, 0.0)
        within = jnp.einsum('hts,shv->thv', scores, value_block_rows, precision=highest_accuracy)
        across_blocks = jnp.einsum('pjy,jyr->pjr', query_block_rows * jnp.exp(cumulative_log), recurrent_state_matrix, precision=highest_accuracy)
        recurrent_state_matrix = jnp.exp(block_final_row)[..., None] * recurrent_state_matrix + jnp.einsum('jnz,jne->nze', scaled_key_rows, value_block_rows, precision=highest_accuracy)
        return (recurrent_state_matrix, within + across_blocks)
    initial = jnp.zeros((RECURRENT_HEADS, KEY_DIM, VAL_DIM), jnp.float32)
    final_state, outputs = lax.scan(advance, initial, (queries, key_decay_rates, values, forget_log_factor))
    recurrent = outputs.reshape(length, RECURRENT_HEADS, VAL_DIM)
    factor = lax.rsqrt(lax.optimization_barrier(jnp.mean(recurrent * recurrent, axis=-1, keepdims=True)) + epsilon)
    normed = (recurrent * factor * head_output_gain.reshape(RECURRENT_HEADS, VAL_DIM)).reshape(length, RECURRENT_HEADS * VAL_DIM)
    mixed = (normed * jax.nn.silu(output_gate_preactivation.astype(jnp.float32))).astype(jnp.bfloat16)
    return jnp.dot(mixed, mixer_output_weight, preferred_element_type=jnp.float32).astype(jnp.bfloat16)

def expert_part(second_batch_tokens, feedforward_norm_gain, chosen_expert_index, chosen_expert_weight, expert_gate_weight, expert_up_weight, expert_down_weight):
    total_rows = second_batch_tokens.shape[0]
    width = second_batch_tokens.shape[1]
    tokens_float = second_batch_tokens.astype(jnp.float32)
    factor = lax.rsqrt(lax.optimization_barrier(jnp.mean(tokens_float * tokens_float, axis=-1, keepdims=True)) + epsilon)
    normed = (tokens_float * factor * feedforward_norm_gain).astype(jnp.bfloat16)
    nsub = total_rows // SUB_B
    blocks = chosen_expert_index.reshape(nsub, SUB_B, TOPK)
    slot_ids = slot_positions(blocks)
    sub_index = jnp.arange(nsub, dtype=jnp.int32)[:, None, None]
    flat_slot = (blocks * nsub + sub_index) * CAP + slot_ids
    token_ids = jnp.broadcast_to(jnp.arange(total_rows, dtype=jnp.int32).reshape(nsub, SUB_B, 1), blocks.shape)
    lookup = jnp.full((EXPERTS * nsub * CAP,), -1, jnp.int32).at[flat_slot.reshape(-1)].set(token_ids.reshape(-1))
    lookup = lookup.reshape(EXPERTS, nsub * CAP)

    def one_expert(inputs):
        row_index, gate_weight, up_weight, down_weight = inputs
        picked = normed[jnp.maximum(row_index, 0)]
        routed = jnp.where((row_index >= 0)[:, None], picked, jnp.zeros((), jnp.bfloat16))
        gate_part = jnp.dot(routed, gate_weight, preferred_element_type=jnp.float32)
        up_part = jnp.dot(routed, up_weight, preferred_element_type=jnp.float32)
        hidden = (jax.nn.silu(gate_part) * up_part).astype(jnp.bfloat16)
        hidden_groups = jnp.transpose(hidden.reshape(-1, N_TP, FFE_DEV), (1, 0, 2))
        down_groups = down_weight.reshape(N_TP, FFE_DEV, width)

        def add_group(running, pair):
            product = jnp.dot(pair[0], pair[1], preferred_element_type=jnp.float32)
            return (running + lax.optimization_barrier(product.astype(jnp.bfloat16)).astype(jnp.float32), None)
        running, unused = lax.scan(add_group, jnp.zeros((hidden.shape[0], width), jnp.float32), (hidden_groups, down_groups))
        return running.astype(jnp.bfloat16)
    outputs = lax.map(one_expert, (lookup, expert_gate_weight, expert_up_weight, expert_down_weight))
    flat_outputs = outputs.reshape(-1, width)
    flat_index = flat_slot.reshape(total_rows, TOPK)
    combined = jnp.zeros((total_rows, width), jnp.float32)
    for ranked in range(TOPK):
        combined = combined + flat_outputs[flat_index[:, ranked]].astype(jnp.float32) * chosen_expert_weight[:, ranked:ranked + 1]
    return combined.astype(jnp.bfloat16)

def reference(query_preactivation, forget_preactivation, value_input_rows, output_gate_preactivation, forget_floor_gap, extra_log_forget, head_output_gain, mixer_output_weight, second_batch_tokens, feedforward_norm_gain, chosen_expert_index, chosen_expert_weight, expert_gate_weight, expert_up_weight, expert_down_weight):
    mixer_output_first = mixer_portion(query_preactivation, forget_preactivation, value_input_rows, output_gate_preactivation, forget_floor_gap, extra_log_forget, head_output_gain, mixer_output_weight)
    moe_out = expert_part(second_batch_tokens, feedforward_norm_gain, chosen_expert_index, chosen_expert_weight, expert_gate_weight, expert_up_weight, expert_down_weight)
    return (mixer_output_first, moe_out)
```

```python
import functools

import jax
import jax.numpy as jnp
from jax import lax
from jax.experimental import pallas as pl
from jax.experimental.pallas import tpu as pltpu
from jax.sharding import PartitionSpec as P

KEY_DIM = 128
VAL_DIM = 64
BLOCK_POSITIONS = 64
TOPK = 2


epsilon = 1e-06


CHUNK = 256
NT = (((1,), (1,)), ((), ()))
TN = (((0,), (0,)), ((), ()))


def local_kernel(heads, q_ref, f_ref, v_ref, gap_ref, extra_ref, rec_ref, qdec_ref, carry_ref, state, base):
    step = pl.program_id(0)

    @pl.when(step == 0)
    def _():
        state[...] = jnp.zeros_like(state)
        base[...] = jnp.zeros_like(base)

    rows, vals = v_ref.shape
    q = q_ref[...].astype(jnp.float32)
    q = q / (1.0 + jnp.exp(-q))
    key = gap_ref[...] / (1.0 + jnp.exp(f_ref[...].astype(jnp.float32)))
    extra = extra_ref[...]
    log_forget = jnp.log(1.0 - key) + jnp.concatenate(
        [jnp.broadcast_to(extra[:, h : h + 1], (rows, KEY_DIM)) for h in range(heads)], axis=1
    )
    at = lax.broadcasted_iota(jnp.int32, (rows, rows), 0)
    of = lax.broadcasted_iota(jnp.int32, (rows, rows), 1)
    lower = jnp.where((at >= of) & (at // BLOCK_POSITIONS == of // BLOCK_POSITIONS), 1.0, 0.0)
    lower = lower.astype(jnp.bfloat16)
    high = log_forget.astype(jnp.bfloat16)
    low = (log_forget - high.astype(jnp.float32)).astype(jnp.bfloat16)
    cumulative = jnp.dot(lower, high, preferred_element_type=jnp.float32) + jnp.dot(
        lower, low, preferred_element_type=jnp.float32
    )
    causal = lax.broadcasted_iota(
        jnp.int32, (BLOCK_POSITIONS, BLOCK_POSITIONS), 0
    ) >= lax.broadcasted_iota(jnp.int32, (BLOCK_POSITIONS, BLOCK_POSITIONS), 1)
    lane_head = lax.broadcasted_iota(jnp.int32, (BLOCK_POSITIONS, vals), 1) // VAL_DIM
    held = [state[h] for h in range(heads)]
    before = base[...]
    half = BLOCK_POSITIONS // 2
    for b in range(rows // BLOCK_POSITIONS):
        part = slice(b * BLOCK_POSITIONS, (b + 1) * BLOCK_POSITIONS)
        cum = cumulative[part]
        mid, last = cum[half - 1 : half], cum[BLOCK_POSITIONS - 1 :]
        q_part = q[part]
        q_mid = (q_part * jnp.exp(cum - mid)).astype(jnp.bfloat16)
        k_mid = (key[part] * jnp.exp(mid - cum)).astype(jnp.bfloat16)
        qdec_ref[part, :] = (q_part * jnp.exp(cum + before)).astype(jnp.bfloat16)
        decay_mid, decay_last, decay_rest = jnp.exp(mid), jnp.exp(last), jnp.exp(last - mid)
        before = before + last
        values = v_ref[part, :]
        out = jnp.zeros((BLOCK_POSITIONS, vals), jnp.float32)
        for h in range(heads):
            lanes = slice(h * KEY_DIM, (h + 1) * KEY_DIM)
            across = lax.dot_general(
                q_mid[:, lanes],
                (held[h] * decay_mid[:, lanes]).astype(jnp.bfloat16),
                NT,
                preferred_element_type=jnp.float32,
            )
            scores = lax.dot_general(
                q_mid[:, lanes], k_mid[:, lanes], NT, preferred_element_type=jnp.float32
            )
            scores = jnp.where(causal, scores, 0.0).astype(jnp.bfloat16)
            within = jnp.dot(scores, values, preferred_element_type=jnp.float32)
            out = jnp.where(lane_head == h, within + across, out)
            update = lax.dot_general(
                values, k_mid[:, lanes], TN, preferred_element_type=jnp.float32
            )
            held[h] = held[h] * decay_last[:, lanes] + update * decay_rest[:, lanes]
        rec_ref[part, :] = out
    for h in range(heads):
        state[h] = held[h]
    base[...] = before

    @pl.when(step == pl.num_programs(0) - 1)
    def _():
        own = [held[h][h * VAL_DIM : (h + 1) * VAL_DIM] for h in range(heads)]
        carry_ref[:VAL_DIM, :] = jnp.concatenate(own, axis=1).astype(jnp.bfloat16)
        total = jnp.exp(before)
        carry_ref[VAL_DIM:, :] = jnp.broadcast_to(total, (16, total.shape[1])).astype(jnp.bfloat16)


def local_recurrence(query, forget, values, gap, extra):
    length, keys = query.shape
    heads, vals = keys // KEY_DIM, values.shape[1]

    def chunk(width):
        return pl.BlockSpec((CHUNK, width), lambda i: (i, 0))

    return pl.pallas_call(
        functools.partial(local_kernel, heads),
        grid=(length // CHUNK,),
        in_specs=[
            chunk(keys),
            chunk(keys),
            chunk(vals),
            pl.BlockSpec((1, keys), lambda i: (0, 0)),
            chunk(heads),
        ],
        out_specs=[
            chunk(vals),
            chunk(keys),
            pl.BlockSpec((VAL_DIM + 16, keys), lambda i: (0, 0)),
        ],
        out_shape=[
            jax.ShapeDtypeStruct((length, vals), jnp.float32),
            jax.ShapeDtypeStruct((length, keys), jnp.bfloat16),
            jax.ShapeDtypeStruct((VAL_DIM + 16, keys), jnp.bfloat16),
        ],
        scratch_shapes=[
            pltpu.VMEM((heads, vals, KEY_DIM), jnp.float32),
            pltpu.VMEM((1, keys), jnp.float32),
        ],
        cost_estimate=pl.CostEstimate(
            flops=10_000_000_000, bytes_accessed=6_000_000, transcendentals=3_000_000
        ),
        name="local_recurrence",
    )(query, forget, values, gap.reshape(1, keys), extra)


def gate_kernel(heads, places, place_ref, rec_ref, qdec_ref, carry_ref, gain_ref, gate_ref, out_ref, held):
    rows, vals = rec_ref.shape

    @pl.when(pl.program_id(0) == 0)
    def _():
        place = place_ref[0]
        total = jnp.zeros((VAL_DIM, heads * KEY_DIM), jnp.float32)
        for i in range(places):
            decay = carry_ref[i, VAL_DIM:, :].astype(jnp.float32)[:1]
            joined = total * decay + carry_ref[i, :VAL_DIM, :].astype(jnp.float32)
            total = jnp.where(i < place, joined, total)
        lane_head = lax.broadcasted_iota(jnp.int32, total.shape, 1) // KEY_DIM
        for h in range(heads):
            held[h * VAL_DIM : (h + 1) * VAL_DIM, :] = jnp.where(lane_head == h, total, 0.0).astype(
                jnp.bfloat16
            )

    rec = rec_ref[...] + lax.dot_general(
        qdec_ref[...], held[...], NT, preferred_element_type=jnp.float32
    )
    at = lax.broadcasted_iota(jnp.int32, (vals, vals), 0) // VAL_DIM
    of = lax.broadcasted_iota(jnp.int32, (vals, vals), 1) // VAL_DIM
    average = jnp.where(at == of, 1.0 / VAL_DIM, 0.0).astype(jnp.bfloat16)
    square = rec * rec
    high = square.astype(jnp.bfloat16)
    low = (square - high.astype(jnp.float32)).astype(jnp.bfloat16)
    mean = jnp.dot(high, average, preferred_element_type=jnp.float32) + jnp.dot(
        low, average, preferred_element_type=jnp.float32
    )
    gate = gate_ref[...].astype(jnp.float32)
    gate = gate / (1.0 + jnp.exp(-gate))
    out_ref[...] = (rec * lax.rsqrt(mean + epsilon) * gain_ref[...] * gate).astype(jnp.bfloat16)


def gated_output(rec, qdec, carries, gain, gate):
    length, vals = rec.shape
    keys = qdec.shape[1]
    heads = keys // KEY_DIM
    rows = 2 * CHUNK

    def chunk(width):
        return pl.BlockSpec((rows, width), lambda i: (i, 0))

    return pl.pallas_call(
        functools.partial(gate_kernel, heads, carries.shape[0]),
        grid=(length // rows,),
        in_specs=[
            pl.BlockSpec(memory_space=pltpu.SMEM),
            chunk(vals),
            chunk(keys),
            pl.BlockSpec(carries.shape, lambda i: (0, 0, 0)),
            pl.BlockSpec((1, vals), lambda i: (0, 0)),
            chunk(vals),
        ],
        out_specs=chunk(vals),
        out_shape=jax.ShapeDtypeStruct((length, vals), jnp.bfloat16),
        scratch_shapes=[pltpu.VMEM((vals, keys), jnp.bfloat16)],
        cost_estimate=pl.CostEstimate(
            flops=2_000_000_000, bytes_accessed=3_000_000, transcendentals=1_000_000
        ),
        name="gated_output",
    )(lax.axis_index("ep").reshape(1), rec, qdec, carries, gain.reshape(1, vals), gate)


def norm_rows(tokens, row_gain):
    tokens_float = tokens.astype(jnp.float32)
    factor = lax.rsqrt(jnp.mean(tokens_float * tokens_float, axis=-1, keepdims=True) + epsilon)
    return (tokens_float * factor * row_gain).astype(jnp.bfloat16)


def slot_positions(blocks, experts_all):
    flattened = blocks.reshape(blocks.shape[0], -1)
    onehot = (flattened[..., None] == jnp.arange(experts_all, dtype=jnp.int32)).astype(jnp.int32)
    earlier = jnp.cumsum(onehot, axis=1) - onehot
    return jnp.sum(earlier * onehot, axis=-1).reshape(blocks.shape)


def fill_slots(rows_in, blocks, slot_ids, experts_all, capacity):
    groups = blocks.shape[0]
    sub_rows = blocks.shape[1]
    group_ids = jnp.arange(groups, dtype=jnp.int32)[:, None, None]
    target = (group_ids * experts_all + blocks) * capacity + slot_ids
    sources = jnp.broadcast_to(
        jnp.arange(sub_rows, dtype=jnp.int32)[None, :, None] + group_ids * sub_rows, blocks.shape
    )
    lookup = (
        jnp.full((groups * experts_all * capacity,), -1, jnp.int32)
        .at[target.reshape(-1)]
        .set(sources.reshape(-1))
    )
    gathered = rows_in.reshape(groups * sub_rows, -1)[jnp.maximum(lookup, 0)]
    filled = jnp.where((lookup >= 0)[:, None], gathered, jnp.zeros((), gathered.dtype))
    return filled.reshape(groups, experts_all, capacity, -1)


def general(
    query_preactivation,
    forget_preactivation,
    value_input_rows,
    output_gate_preactivation,
    forget_floor_gap,
    extra_log_forget,
    head_output_gain,
    mixer_output_weight,
    second_batch_tokens,
    feedforward_norm_gain,
    chosen_expert_index,
    chosen_expert_weight,
    expert_gate_weight,
    expert_up_weight,
    expert_down_weight,
):
    local_experts = expert_gate_weight.shape[0]
    places = lax.axis_size("ep")
    experts_all = local_experts * places
    groups = lax.axis_size("tp")
    width = second_batch_tokens.shape[1]
    sub_rows = second_batch_tokens.shape[0] // groups
    capacity = max(2, sub_rows * TOPK * 5 // (4 * experts_all))
    place = lax.axis_index("ep")
    position = lax.axis_index("tp")
    pairs = groups // 2
    side = lax.rem(position, 2)

    all_routes = chosen_expert_index.reshape(pairs, 2, sub_rows, TOPK)
    routes = lax.dynamic_index_in_dim(all_routes, side, 1, False)
    all_tokens = second_batch_tokens.reshape(pairs, 2, sub_rows, width)
    tokens = lax.dynamic_index_in_dim(all_tokens, side, 1, False)
    slots = slot_positions(routes, experts_all)
    outgoing = fill_slots(
        norm_rows(tokens, feedforward_norm_gain), routes, slots, experts_all, capacity
    )
    outgoing, query_preactivation = lax.optimization_barrier((outgoing, query_preactivation))
    outgoing = outgoing.reshape(pairs, places, local_experts, capacity, width)
    arrived = []
    for step in range(places):
        block = lax.dynamic_index_in_dim(outgoing, place ^ step, 1, False)
        if step:
            block = lax.ppermute(block, "ep", [(i, i ^ step) for i in range(places)])
        arrived.append(block)
    partners = [(i, i ^ 1) for i in range(groups)]
    shape = (pairs, places, local_experts, capacity, width)
    others = [lax.ppermute(block, "tp", partners) for block in arrived]
    own_side = jnp.stack(arrived, axis=1)
    other_side = jnp.stack(others, axis=1)

    recurrent, query_decayed, carry = local_recurrence(
        query_preactivation,
        forget_preactivation,
        value_input_rows,
        forget_floor_gap,
        extra_log_forget,
    )
    carries = lax.all_gather(carry, "ep")
    mixed = gated_output(
        recurrent, query_decayed, carries, head_output_gain, output_gate_preactivation
    )
    mixed_all = lax.all_gather(mixed, "tp", axis=1, tiled=True)

    def experts(rows):
        gate_part = jnp.einsum(
            "tsecd,edf->tsecf", rows, expert_gate_weight, preferred_element_type=jnp.float32
        )
        up_part = jnp.einsum(
            "tsecd,edf->tsecf", rows, expert_up_weight, preferred_element_type=jnp.float32
        )
        hidden = (jax.nn.silu(gate_part) * up_part).astype(jnp.bfloat16)
        product = jnp.einsum(
            "tsecf,efd->tsecd", hidden, expert_down_weight, preferred_element_type=jnp.float32
        )
        return product.astype(jnp.bfloat16)

    other_side, mixed = lax.optimization_barrier((other_side, mixed))
    for_partner = experts(other_side)
    own_side, for_partner = lax.optimization_barrier((own_side, for_partner))
    from_partner = lax.ppermute(for_partner, "tp", partners)
    product = experts(own_side).astype(jnp.float32) + from_partner.astype(jnp.float32)
    product, mixed_all = lax.optimization_barrier((product.astype(jnp.bfloat16), mixed_all))
    to_return = lax.psum_scatter(
        product,
        "tp",
        scatter_dimension=0,
        tiled=True,
        axis_index_groups=[list(range(c, groups, 2)) for c in range(2)],
    )
    to_return = to_return.reshape(shape[1:])
    mixer_output_first = jnp.dot(
        mixed_all, mixer_output_weight, preferred_element_type=jnp.float32
    ).astype(jnp.bfloat16)
    returned = []
    for step in range(places):
        block = to_return[step]
        if step:
            block = lax.ppermute(block, "ep", [(i, i ^ step) for i in range(places)])
        returned.append(block)
    results = jnp.concatenate(returned, axis=0).reshape(experts_all * capacity, width)
    own_routes = lax.dynamic_index_in_dim(routes, position // 2, 0, False)
    own_slots = lax.dynamic_index_in_dim(slots, position // 2, 0, False)
    own_weights = lax.dynamic_slice_in_dim(chosen_expert_weight, position * sub_rows, sub_rows, 0)
    holder = (own_routes // local_experts) ^ place
    flat_index = (holder * local_experts + own_routes % local_experts) * capacity + own_slots
    combined = jnp.zeros((sub_rows, width), jnp.float32)
    for ranked in range(TOPK):
        combined = (
            combined
            + results[flat_index[:, ranked]].astype(jnp.float32)
            * own_weights[:, ranked : ranked + 1]
        )
    return (mixer_output_first, combined.astype(jnp.bfloat16))


MESH = pl.DeviceIdType.MESH
LANES = 128
ROW_CHUNKS = 4


def fused_kernel(
    idx_ref, weight_ref, norm_gain_ref, gap_ref, extra_ref, head_gain_ref,
    tok_hbm, q_hbm, f_hbm, v_hbm, g_hbm, wo_hbm, wg_hbm, wu_hbm, wd_hbm,
    out_ref, moe_ref,
    tok, q, f, v, gate, wo, wgu, wd,
    send_rows, rows, hidden, pair_out, pair_in, psum, from_end, from_mate, from_inner,
    result_out, results, combined, moe_buf,
    state, base, carries, rec, qdec, held_state, mixed_all, out_acc,
    load_sem, disp_send, disp_recv, dfwd_send, dfwd_recv, pair_send, pair_recv,
    end_send, end_recv, mate_send, mate_recv, inner_send, inner_recv,
    ret_send, ret_recv, swap_send, swap_recv, carry_send, carry_recv,
    own_send, own_recv, ag_send, ag_recv, agf_send, agf_recv,
):
    f32, bf16 = jnp.float32, jnp.bfloat16
    ep = lax.axis_index("ep")
    tp = lax.axis_index("tp")
    z, c = tp // 2, tp % 2
    oc = 1 - c
    mate = z + 1 - 2 * (z % 2)
    is_end = (z == 0) | (z == 3)
    is_inner = (z == 1) | (z == 2)
    places = rows.shape[0]
    steps = places
    pairs = mixed_all.shape[0]
    two = idx_ref.shape[1] // pairs
    sub = two // 2
    width = tok.shape[1]
    hw = width // 2
    rows_all = rows.shape[1]
    cp = rows_all // pairs
    cap = cp // 2
    length, keys = q.shape
    vals = v.shape[1]
    heads = keys // KEY_DIM
    blocks_f = wgu.shape[0]
    vc = vals
    ep_peer = [{"ep": ep ^ s} for s in range(places)]
    z_peer = [{"tp": (z ^ x) * 2 + c} for x in range(pairs)]
    partner = {"tp": z * 2 + oc}
    mate_dev = {"tp": mate * 2 + c}
    across_dev = {"tp": (pairs - 1 - z) * 2 + c}

    def half(i):
        return pl.ds(pl.multiple_of(i * hw, LANES), hw)

    def vcols(i):
        return pl.ds(pl.multiple_of(i * vc, LANES), vc)

    def zrows(d, n=1):
        return pl.ds(pl.multiple_of(d * cp, 16), n * cp)

    def remote(src, dst, ssem, rsem, dev):
        return pltpu.make_async_remote_copy(
            src_ref=src, dst_ref=dst, send_sem=ssem, recv_sem=rsem, device_id=dev, device_id_type=MESH
        )

    loads = {}

    def load(name, src, dst):
        copy = pltpu.make_async_copy(src, dst, load_sem.at[len(loads)])
        copy.start()
        loads[name] = copy

    for g in range(pairs):
        part = pl.ds(g * two, two)
        load(("tok", g), tok_hbm.at[part], tok.at[part])
    for j in range(blocks_f):
        cols = pl.ds(j * LANES, LANES)
        load(("wg", j), wg_hbm.at[0, :, cols], wgu.at[j, :, pl.ds(0, LANES)])
        load(("wu", j), wu_hbm.at[0, :, cols], wgu.at[j, :, pl.ds(LANES, LANES)])
    load("wd", wd_hbm.at[0], wd)
    load("q", q_hbm, q)
    load("f", f_hbm, f)
    load("v", v_hbm, v)
    load("gate", g_hbm, gate)
    load("wo", wo_hbm, wo)

    barrier = pltpu.get_barrier_semaphore()
    greet = ep_peer[1:] + z_peer[1:] + [partner]
    for dev in greet:
        pl.semaphore_signal(barrier, inc=1, device_id=dev, device_id_type=MESH)

    tri_a = lax.broadcasted_iota(jnp.int32, (two, two), 0)
    tri_b = lax.broadcasted_iota(jnp.int32, (two, two), 1)
    earlier = jnp.where((tri_a < tri_b) & (tri_a // sub == tri_b // sub), 1.0, 0.0).astype(bf16)
    lane_side = lax.broadcasted_iota(jnp.int32, (8, two), 1) // sub
    slot_row = lax.broadcasted_iota(jnp.int32, (cp, two), 0).astype(f32)
    expert_row = ep ^ lax.broadcasted_iota(jnp.int32, (8, two), 0)

    def targets(lanes):
        first = jnp.broadcast_to(idx_ref[0:1, lanes], (8, two)) == expert_row
        second = jnp.broadcast_to(idx_ref[1:2, lanes], (8, two)) == expert_row
        match = first | second
        before = jnp.dot(jnp.where(match, 1.0, 0.0).astype(bf16), earlier, preferred_element_type=f32)
        where_to = jnp.where(match, before + (lane_side * cap).astype(f32), -1.0)
        return where_to, first, second

    for g in range(pairs):
        part = slice(g * two, (g + 1) * two)
        loads[("tok", g)].wait()
        tokens = tok[part, :].astype(f32)
        factor = lax.rsqrt(jnp.mean(tokens * tokens, axis=-1, keepdims=True) + epsilon)
        tok[part, :] = (tokens * factor * norm_gain_ref[...]).astype(bf16)
        where_to, _, _ = targets(slice(g * two, (g + 1) * two))
        onehots = [
            jnp.where(slot_row == where_to[s : s + 1, :], 1.0, 0.0).astype(bf16) for s in range(places)
        ]
        rows[0, g * cp : (g + 1) * cp, :] = jnp.dot(
            onehots[0], tok[part, :], preferred_element_type=f32
        ).astype(bf16)
        own_half = tok[part, half(c)]
        for s in range(1, places):
            send_rows[s - 1, g * cp : (g + 1) * cp, :] = jnp.dot(
                onehots[s], own_half, preferred_element_type=f32
            ).astype(bf16)

    pl.semaphore_wait(barrier, len(greet))

    def dispatch(s):
        return remote(
            send_rows.at[s - 1], rows.at[s, :, half(c)], disp_send.at[s - 1], disp_recv.at[s - 1], ep_peer[s]
        )

    def dispatch_forward(s):
        return remote(
            rows.at[s, :, half(c)], rows.at[s, :, half(c)], dfwd_send.at[s - 1], dfwd_recv.at[s - 1], partner
        )

    def dispatch_forward_in(s):
        return remote(
            rows.at[s, :, half(oc)], rows.at[s, :, half(oc)], dfwd_send.at[s - 1], dfwd_recv.at[s - 1], partner
        )

    for s in range(1, places):
        dispatch(s).start()

    def forward(s):
        dispatch(s).wait_recv()
        dispatch_forward(s).start()

    def pair_copy(s):
        return remote(pair_out.at[s], pair_in.at[s], pair_send.at[s], pair_recv.at[s], partner)

    def moe(s):
        if s:
            dispatch_forward_in(s).wait_recv()

        def gate_up(j, _):
            acc = jnp.dot(rows[s], wgu[j], preferred_element_type=f32)
            part, up = acc[:, :LANES], acc[:, LANES:]
            value = part / (1.0 + jnp.exp(-part)) * up
            hidden[:, pl.ds(pl.multiple_of(j * LANES, LANES), LANES)] = value.astype(bf16)
            return 0

        lax.fori_loop(0, blocks_f, gate_up, 0)
        tile = min(256, hw)

        def down(dst, side):
            def body(j, _):
                start = pl.multiple_of(side * hw + j * tile, LANES)
                acc = jnp.dot(hidden[...], wd[:, pl.ds(start, tile)], preferred_element_type=f32)
                dst[s, :, pl.ds(pl.multiple_of(j * tile, LANES), tile)] = acc.astype(bf16)
                return 0

            lax.fori_loop(0, hw // tile, body, 0)

        if s == 0:
            loads["wd"].wait()
        down(pair_out, oc)
        pair_copy(s).start()
        down(psum, c)

    far = (1 - z // 2) * 2

    def end_copy(s):
        return remote(psum.at[s, zrows(far, 2)], from_end.at[s], end_send.at[s], end_recv.at[s], mate_dev)

    def mate_copy(s):
        return remote(psum.at[s, zrows(mate)], from_mate.at[s], mate_send.at[s], mate_recv.at[s], mate_dev)

    def inner_copy(s):
        return remote(psum.at[s, zrows(far, 2)], from_inner.at[s], inner_send.at[s], inner_recv.at[s], across_dev)

    def add_into(s, at, other):
        psum[s, at, :] = (psum[s, at, :].astype(f32) + other.astype(f32)).astype(bf16)

    def stage1(s):
        pair_copy(s).wait_recv()

        def body(k, _):
            at = zrows(k)
            add_into(s, at, pair_in[s, at, :])
            return 0

        lax.fori_loop(0, pairs, body, 0)

        @pl.when(is_end)
        def _():
            end_copy(s).start()
            mate_copy(s).start()

    def stage2(s):
        @pl.when(is_inner)
        def _():
            end_copy(s).wait_recv()

            def body(k, _):
                add_into(s, zrows(far + k), from_end[s, zrows(k), :])
                return 0

            lax.fori_loop(0, 2, body, 0)
            inner_copy(s).start()

    def stage3(s):
        @pl.when(is_inner)
        def _():
            inner_copy(s).wait_recv()
            add_into(s, zrows(mate), from_inner[s, zrows(mate % 2), :])
            mate_copy(s).start()

    def result_copy(s):
        return remote(
            result_out.at[s], results.at[pl.ds(s * cp, cp)], ret_send.at[s - 1], ret_recv.at[s - 1], ep_peer[s]
        )

    def stage4(s):
        mate_copy(s).wait_recv()
        total = psum[s, zrows(z), :].astype(f32) + from_mate[s].astype(f32)
        here = slice(s * cp, (s + 1) * cp)

        def put(value):
            if s:
                result_out[s] = value.astype(bf16)
            else:
                results[here, :] = value.astype(bf16)

        @pl.when(is_end)
        def _():
            put(total)

        @pl.when(is_inner)
        def _():
            put(total + from_inner[s, zrows(z % 2), :].astype(f32))

        if s:
            result_copy(s).start()

    def carry_copy(s):
        return remote(carries.at[0], carries.at[s], carry_send.at[s - 1], carry_recv.at[s - 1], ep_peer[s])

    def recurrence(services):
        state[...] = jnp.zeros_like(state)
        base[...] = jnp.zeros_like(base)
        n = CHUNK
        at = lax.broadcasted_iota(jnp.int32, (n, n), 0)
        of = lax.broadcasted_iota(jnp.int32, (n, n), 1)
        same = (at >= of) & (at // BLOCK_POSITIONS == of // BLOCK_POSITIONS)
        lower = jnp.where(same, 1.0, 0.0).astype(bf16)
        er = lax.broadcasted_iota(jnp.int32, (8, n), 0)
        pick_row = lax.broadcasted_iota(jnp.int32, (8, keys), 0)
        pick_head = lax.broadcasted_iota(jnp.int32, (8, keys), 1) // KEY_DIM
        pick = jnp.where((pick_row % heads == pick_head) & (pick_row < 3 * heads), 1.0, 0.0).astype(bf16)
        small = (BLOCK_POSITIONS, BLOCK_POSITIONS)
        causal = lax.broadcasted_iota(jnp.int32, small, 0) >= lax.broadcasted_iota(jnp.int32, small, 1)
        lane_head = lax.broadcasted_iota(jnp.int32, (BLOCK_POSITIONS, vals), 1) // VAL_DIM

        def chunk(i, _):
            for when, work in services.items():

                @pl.when(i == when)
                def _():
                    work()

            start = pl.multiple_of(i * n, n)
            here = pl.ds(start, n)
            qc = q[here, :].astype(f32)
            qc = qc / (1.0 + jnp.exp(-qc))
            key = gap_ref[...] / (1.0 + jnp.exp(f[here, :].astype(f32)))
            terms = jnp.zeros((8, n), f32)
            for h in range(heads):
                value = jnp.broadcast_to(extra_ref[h : h + 1, here], (8, n))
                one = value.astype(bf16).astype(f32)
                second = (value - one).astype(bf16).astype(f32)
                third = value - one - second
                terms = jnp.where(er == h, one, terms)
                terms = jnp.where(er == heads + h, second, terms)
                terms = jnp.where(er == 2 * heads + h, third, terms)
            extra = lax.dot_general(terms.astype(bf16), pick, TN, preferred_element_type=f32)
            log_forget = jnp.log(1.0 - key) + extra
            high = log_forget.astype(bf16)
            low = (log_forget - high.astype(f32)).astype(bf16)
            cumulative = jnp.dot(lower, high, preferred_element_type=f32) + jnp.dot(
                lower, low, preferred_element_type=f32
            )
            held = [state[h] for h in range(heads)]
            before = base[...]
            mid_at = BLOCK_POSITIONS // 2
            for b in range(n // BLOCK_POSITIONS):
                part = slice(b * BLOCK_POSITIONS, (b + 1) * BLOCK_POSITIONS)
                block = pl.ds(start + b * BLOCK_POSITIONS, BLOCK_POSITIONS)
                cum = cumulative[part]
                mid, last = cum[mid_at - 1 : mid_at], cum[BLOCK_POSITIONS - 1 :]
                q_part = qc[part]
                q_mid = (q_part * jnp.exp(cum - mid)).astype(bf16)
                k_mid = (key[part] * jnp.exp(mid - cum)).astype(bf16)
                qdec[block, :] = (q_part * jnp.exp(cum + before)).astype(bf16)
                decay_mid, decay_last, decay_rest = jnp.exp(mid), jnp.exp(last), jnp.exp(last - mid)
                before = before + last
                values = v[block, :]
                out = jnp.zeros((BLOCK_POSITIONS, vals), f32)
                for h in range(heads):
                    lanes = slice(h * KEY_DIM, (h + 1) * KEY_DIM)
                    across = lax.dot_general(
                        q_mid[:, lanes],
                        (held[h] * decay_mid[:, lanes]).astype(bf16),
                        NT,
                        preferred_element_type=f32,
                    )
                    scores = lax.dot_general(q_mid[:, lanes], k_mid[:, lanes], NT, preferred_element_type=f32)
                    scores = jnp.where(causal, scores, 0.0).astype(bf16)
                    within = jnp.dot(scores, values, preferred_element_type=f32)
                    out = jnp.where(lane_head == h, within + across, out)
                    update = lax.dot_general(values, k_mid[:, lanes], TN, preferred_element_type=f32)
                    held[h] = held[h] * decay_last[:, lanes] + update * decay_rest[:, lanes]
                rec[block, :] = out
            for h in range(heads):
                state[h] = held[h]
            base[...] = before
            return 0

        lax.fori_loop(0, length // n, chunk, 0)
        own = [state[h, h * VAL_DIM : (h + 1) * VAL_DIM, :] for h in range(heads)]
        carries[0, :VAL_DIM, :] = jnp.concatenate(own, axis=1).astype(bf16)
        total = jnp.exp(base[...])
        carries[0, VAL_DIM:, :] = jnp.broadcast_to(total, (16, keys)).astype(bf16)
        for s in range(1, places):
            carry_copy(s).start()

    chunk_rows = length // ROW_CHUNKS

    def rows_of(r):
        return pl.ds(r * chunk_rows, chunk_rows)

    def own_copy(r):
        here = mixed_all.at[z, rows_of(r), vcols(c)]
        return remote(here, here, own_send.at[r], own_recv.at[r], partner)

    def own_in(r):
        here = mixed_all.at[z, rows_of(r), vcols(oc)]
        return remote(here, here, own_send.at[r], own_recv.at[r], partner)

    def ag_copy(x, r):
        here = mixed_all.at[z, rows_of(r), vcols(c)]
        return remote(here, here, ag_send.at[x - 1, r], ag_recv.at[x - 1, r], z_peer[x])

    def ag_in(x, r):
        here = mixed_all.at[z ^ x, rows_of(r), vcols(c)]
        return remote(here, here, ag_send.at[x - 1, r], ag_recv.at[x - 1, r], z_peer[x])

    def ag_forward(x, r):
        here = mixed_all.at[z ^ x, rows_of(r), vcols(c)]
        return remote(here, here, agf_send.at[x - 1, r], agf_recv.at[x - 1, r], partner)

    def ag_forward_in(x, r):
        here = mixed_all.at[z ^ x, rows_of(r), vcols(oc)]
        return remote(here, here, agf_send.at[x - 1, r], agf_recv.at[x - 1, r], partner)

    def gated():
        for s in range(1, places):
            carry_copy(s).wait_recv()
        total = jnp.zeros((VAL_DIM, keys), f32)
        for i in range(places):
            decay = carries[ep ^ i, VAL_DIM:, :].astype(f32)[:1]
            joined = total * decay + carries[ep ^ i, :VAL_DIM, :].astype(f32)
            total = jnp.where(i < ep, joined, total)
        lane_head = lax.broadcasted_iota(jnp.int32, total.shape, 1) // KEY_DIM
        for h in range(heads):
            held_state[h * VAL_DIM : (h + 1) * VAL_DIM, :] = jnp.where(lane_head == h, total, 0.0).astype(bf16)
        at = lax.broadcasted_iota(jnp.int32, (vals, vals), 0) // VAL_DIM
        of = lax.broadcasted_iota(jnp.int32, (vals, vals), 1) // VAL_DIM
        average = jnp.where(at == of, 1.0 / VAL_DIM, 0.0).astype(bf16)
        for r in range(ROW_CHUNKS):
            here = rows_of(r)
            whole = rec[here, :] + lax.dot_general(
                qdec[here, :], held_state[...], NT, preferred_element_type=f32
            )
            square = whole * whole
            high = square.astype(bf16)
            low = (square - high.astype(f32)).astype(bf16)
            mean = jnp.dot(high, average, preferred_element_type=f32) + jnp.dot(
                low, average, preferred_element_type=f32
            )
            opened = gate[here, :].astype(f32)
            opened = opened / (1.0 + jnp.exp(-opened))
            mixed = (whole * lax.rsqrt(mean + epsilon) * head_gain_ref[...] * opened).astype(bf16)
            mixed_all[z, here, vcols(c)] = mixed
            for x in range(1, pairs):
                ag_copy(x, r).start()
            own_copy(r).start()

    def project(x, last):
        kw = 2 * vc
        weight = wo[pl.ds(pl.multiple_of((z ^ x) * kw, LANES), kw), :]
        for r in range(ROW_CHUNKS):
            if x:
                ag_forward_in(x, r).wait_recv()
            else:
                own_in(r).wait_recv()
            here = rows_of(r)
            part = jnp.dot(mixed_all[z ^ x, here, :], weight, preferred_element_type=f32)
            if x:
                part = part + out_acc[here, :]
            if last:
                out_ref[here, :] = part.astype(bf16)
            else:
                out_acc[here, :] = part

    def ag_pass(x):
        for r in range(ROW_CHUNKS):
            ag_in(x, r).wait_recv()
            ag_forward(x, r).start()

    def swap_copy():
        return remote(
            combined.at[pl.ds(pl.multiple_of(oc * sub, 16), sub)],
            moe_buf.at[:, half(c)], swap_send.at[0], swap_recv.at[0], partner,
        )

    def swap_in():
        return remote(
            combined.at[pl.ds(pl.multiple_of(oc * sub, 16), sub)],
            moe_buf.at[:, half(oc)], swap_send.at[0], swap_recv.at[0], partner,
        )

    def combine():
        lanes = pl.ds(pl.multiple_of(z * two, LANES), two)
        where_to, first, second = targets(lanes)
        weight = jnp.where(first, jnp.broadcast_to(weight_ref[0:1, lanes], (8, two)), 0.0) + jnp.where(
            second, jnp.broadcast_to(weight_ref[1:2, lanes], (8, two)), 0.0
        )
        high = weight.astype(bf16).astype(f32)
        low = weight - high
        picks = [slot_row == where_to[s : s + 1, :] for s in range(places)]
        coarse = jnp.concatenate(
            [jnp.where(picks[s], high[s : s + 1, :], 0.0).astype(bf16) for s in range(places)], axis=0
        )
        fine = jnp.concatenate(
            [jnp.where(picks[s], low[s : s + 1, :], 0.0).astype(bf16) for s in range(places)], axis=0
        )
        for s in range(1, places):
            result_copy(s).wait_recv()
        total = lax.dot_general(coarse, results[...], TN, preferred_element_type=f32) + lax.dot_general(
            fine, results[...], TN, preferred_element_type=f32
        )
        combined[...] = total.astype(bf16)
        swap_copy().start()

    def finish():
        moe_buf[:, half(c)] = combined[pl.ds(pl.multiple_of(c * sub, 16), sub), :]
        swap_in().wait_recv()
        moe_ref[...] = moe_buf[...]

    for j in range(blocks_f):
        loads[("wg", j)].wait()
        loads[("wu", j)].wait()
    moe(0)
    for name in ("q", "f", "v"):
        loads[name].wait()
    recurrence(
        {
            1: lambda: stage1(0),
            3: lambda: stage2(0),
            5: lambda: (stage3(0), forward(1)),
            6: lambda: forward(2),
        }
    )
    moe(1)
    stage1(1)
    loads["gate"].wait()
    gated()
    forward(3)
    moe(2)
    stage2(1)
    stage1(2)
    moe(3)
    stage3(1)
    stage2(2)
    stage1(3)
    loads["wo"].wait()
    project(0, False)
    stage4(0)
    stage4(1)
    stage3(2)
    stage2(3)
    ag_pass(1)
    stage4(2)
    project(1, False)
    stage3(3)
    ag_pass(2)
    stage4(3)
    project(2, False)
    ag_pass(3)
    combine()
    project(3, True)
    finish()

    for s in range(1, places):
        dispatch(s).wait_send()
        dispatch_forward(s).wait_send()
        carry_copy(s).wait_send()
        result_copy(s).wait_send()
    for s in range(places):
        pair_copy(s).wait_send()
        mate_copy(s).wait_send()

        @pl.when(is_end)
        def _():
            end_copy(s).wait_send()

        @pl.when(is_inner)
        def _():
            inner_copy(s).wait_send()

    for r in range(ROW_CHUNKS):
        own_copy(r).wait_send()
        for x in range(1, pairs):
            ag_copy(x, r).wait_send()
            ag_forward(x, r).wait_send()
    swap_copy().wait_send()


def on_device(*arrays):
    (
        query, forget, values, gate, gap, extra, head_gain, out_weight,
        tokens, norm_gain, index, weight, gate_weight, up_weight, down_weight,
    ) = arrays
    places, groups = lax.axis_size("ep"), lax.axis_size("tp")
    pairs = groups // 2
    length, keys = query.shape
    vals = values.shape[1]
    count, width = tokens.shape
    hidden = gate_weight.shape[2]
    sub = count // groups
    experts_all = gate_weight.shape[0] * places
    capacity = max(2, sub * TOPK * 5 // (4 * experts_all))
    fits = (
        places == 4
        and groups == 8
        and gate_weight.shape[0] == 1
        and 2 * sub == LANES
        and capacity % 8 == 0
        and capacity <= sub
        and vals == LANES
        and keys == 2 * KEY_DIM
        and length % (ROW_CHUNKS * CHUNK) == 0
        and hidden % LANES == 0
        and width % 512 == 0
    )
    if not fits:
        return general(*arrays)
    heads = keys // KEY_DIM
    cp = 2 * capacity
    rows_all = pairs * cp
    hw = width // 2
    features = out_weight.shape[1]
    bf16, f32 = jnp.bfloat16, jnp.float32
    vmem = pl.BlockSpec(memory_space=pltpu.VMEM)
    anywhere = pl.BlockSpec(memory_space=pl.ANY)
    dma = pltpu.SemaphoreType.DMA
    scratch = [
        pltpu.VMEM((count, width), bf16),
        pltpu.VMEM((length, keys), bf16),
        pltpu.VMEM((length, keys), bf16),
        pltpu.VMEM((length, vals), bf16),
        pltpu.VMEM((length, vals), bf16),
        pltpu.VMEM(out_weight.shape, bf16),
        pltpu.VMEM((hidden // LANES, width, 2 * LANES), bf16),
        pltpu.VMEM((hidden, width), bf16),
        pltpu.VMEM((places - 1, rows_all, hw), bf16),
        pltpu.VMEM((places, rows_all, width), bf16),
        pltpu.VMEM((rows_all, hidden), bf16),
        pltpu.VMEM((places, rows_all, hw), bf16),
        pltpu.VMEM((places, rows_all, hw), bf16),
        pltpu.VMEM((places, rows_all, hw), bf16),
        pltpu.VMEM((places, 2 * cp, hw), bf16),
        pltpu.VMEM((places, cp, hw), bf16),
        pltpu.VMEM((places, 2 * cp, hw), bf16),
        pltpu.VMEM((places, cp, hw), bf16),
        pltpu.VMEM((places * cp, hw), bf16),
        pltpu.VMEM((2 * sub, hw), bf16),
        pltpu.VMEM((sub, width), bf16),
        pltpu.VMEM((heads, vals, KEY_DIM), f32),
        pltpu.VMEM((1, keys), f32),
        pltpu.VMEM((places, VAL_DIM + 16, keys), bf16),
        pltpu.VMEM((length, vals), f32),
        pltpu.VMEM((length, keys), bf16),
        pltpu.VMEM((vals, keys), bf16),
        pltpu.VMEM((pairs, length, 2 * vals), bf16),
        pltpu.VMEM((length, features), f32),
    ]
    n_loads = pairs + 2 * (hidden // LANES) + 6
    peers = places - 1
    sems = [dma((n_loads,))]
    sems += [dma((peers,))] * 4 + [dma((places,))] * 8 + [dma((peers,))] * 2 + [dma((1,))] * 2
    sems += [dma((peers,))] * 2 + [dma((ROW_CHUNKS,))] * 2 + [dma((pairs - 1, ROW_CHUNKS))] * 4
    return pl.pallas_call(
        fused_kernel,
        in_specs=[vmem] * 6 + [anywhere] * 9,
        out_specs=[vmem, vmem],
        out_shape=[
            jax.ShapeDtypeStruct((length, features), bf16),
            jax.ShapeDtypeStruct((sub, width), bf16),
        ],
        scratch_shapes=scratch + sems,
        compiler_params=pltpu.CompilerParams(
            collective_id=0, has_side_effects=True, vmem_limit_bytes=64 * 1024 * 1024 - 65536
        ),
        name="fused_layer",
    )(
        index.T, weight.T, norm_gain.reshape(1, width), gap.reshape(1, keys), extra.T,
        head_gain.reshape(1, vals), tokens, query, forget, values, gate, out_weight,
        gate_weight, up_weight, down_weight,
    )


def solution(mesh):
    placed = (
        P("ep", "tp"),
        P("ep", "tp"),
        P("ep", "tp"),
        P("ep", "tp"),
        P("tp"),
        P("ep", "tp"),
        P("tp"),
        P(None, "tp"),
        P("ep", None),
        P(),
        P("ep", None),
        P("ep", None),
        P("ep", None, "tp"),
        P("ep", None, "tp"),
        P("ep", "tp", None),
    )
    return jax.shard_map(
        on_device,
        mesh=mesh,
        in_specs=placed,
        out_specs=(P("ep", "tp"), P(("ep", "tp"), None)),
        check_vma=False,
    )
```

```python
import functools

import jax
import jax.numpy as jnp
from jax import lax
from jax.experimental import pallas as pl
from jax.experimental.pallas import tpu as pltpu
from jax.sharding import PartitionSpec as P

KEY_DIM = 128
VAL_DIM = 64
BLOCK_POSITIONS = 64
TOPK = 2


epsilon = 1e-06


CHUNK = 256
NT = (((1,), (1,)), ((), ()))
TN = (((0,), (0,)), ((), ()))


def local_kernel(heads, q_ref, f_ref, v_ref, gap_ref, extra_ref, rec_ref, qdec_ref, carry_ref, state, base):
    step = pl.program_id(0)

    @pl.when(step == 0)
    def _():
        state[...] = jnp.zeros_like(state)
        base[...] = jnp.zeros_like(base)

    rows, vals = v_ref.shape
    q = q_ref[...].astype(jnp.float32)
    q = q / (1.0 + jnp.exp(-q))
    key = gap_ref[...] / (1.0 + jnp.exp(f_ref[...].astype(jnp.float32)))
    extra = extra_ref[...]
    log_forget = jnp.log(1.0 - key) + jnp.concatenate(
        [jnp.broadcast_to(extra[:, h : h + 1], (rows, KEY_DIM)) for h in range(heads)], axis=1
    )
    at = lax.broadcasted_iota(jnp.int32, (rows, rows), 0)
    of = lax.broadcasted_iota(jnp.int32, (rows, rows), 1)
    lower = jnp.where((at >= of) & (at // BLOCK_POSITIONS == of // BLOCK_POSITIONS), 1.0, 0.0)
    lower = lower.astype(jnp.bfloat16)
    high = log_forget.astype(jnp.bfloat16)
    low = (log_forget - high.astype(jnp.float32)).astype(jnp.bfloat16)
    cumulative = jnp.dot(lower, high, preferred_element_type=jnp.float32) + jnp.dot(
        lower, low, preferred_element_type=jnp.float32
    )
    causal = lax.broadcasted_iota(
        jnp.int32, (BLOCK_POSITIONS, BLOCK_POSITIONS), 0
    ) >= lax.broadcasted_iota(jnp.int32, (BLOCK_POSITIONS, BLOCK_POSITIONS), 1)
    lane_head = lax.broadcasted_iota(jnp.int32, (BLOCK_POSITIONS, vals), 1) // VAL_DIM
    held = [state[h] for h in range(heads)]
    before = base[...]
    half = BLOCK_POSITIONS // 2
    for b in range(rows // BLOCK_POSITIONS):
        part = slice(b * BLOCK_POSITIONS, (b + 1) * BLOCK_POSITIONS)
        cum = cumulative[part]
        mid, last = cum[half - 1 : half], cum[BLOCK_POSITIONS - 1 :]
        q_part = q[part]
        q_mid = (q_part * jnp.exp(cum - mid)).astype(jnp.bfloat16)
        k_mid = (key[part] * jnp.exp(mid - cum)).astype(jnp.bfloat16)
        qdec_ref[part, :] = (q_part * jnp.exp(cum + before)).astype(jnp.bfloat16)
        decay_mid, decay_last, decay_rest = jnp.exp(mid), jnp.exp(last), jnp.exp(last - mid)
        before = before + last
        values = v_ref[part, :]
        out = jnp.zeros((BLOCK_POSITIONS, vals), jnp.float32)
        for h in range(heads):
            lanes = slice(h * KEY_DIM, (h + 1) * KEY_DIM)
            across = lax.dot_general(
                q_mid[:, lanes],
                (held[h] * decay_mid[:, lanes]).astype(jnp.bfloat16),
                NT,
                preferred_element_type=jnp.float32,
            )
            scores = lax.dot_general(
                q_mid[:, lanes], k_mid[:, lanes], NT, preferred_element_type=jnp.float32
            )
            scores = jnp.where(causal, scores, 0.0).astype(jnp.bfloat16)
            within = jnp.dot(scores, values, preferred_element_type=jnp.float32)
            out = jnp.where(lane_head == h, within + across, out)
            update = lax.dot_general(
                values, k_mid[:, lanes], TN, preferred_element_type=jnp.float32
            )
            held[h] = held[h] * decay_last[:, lanes] + update * decay_rest[:, lanes]
        rec_ref[part, :] = out
    for h in range(heads):
        state[h] = held[h]
    base[...] = before

    @pl.when(step == pl.num_programs(0) - 1)
    def _():
        own = [held[h][h * VAL_DIM : (h + 1) * VAL_DIM] for h in range(heads)]
        carry_ref[:VAL_DIM, :] = jnp.concatenate(own, axis=1).astype(jnp.bfloat16)
        total = jnp.exp(before)
        carry_ref[VAL_DIM:, :] = jnp.broadcast_to(total, (16, total.shape[1])).astype(jnp.bfloat16)


def local_recurrence(query, forget, values, gap, extra):
    length, keys = query.shape
    heads, vals = keys // KEY_DIM, values.shape[1]

    def chunk(width):
        return pl.BlockSpec((CHUNK, width), lambda i: (i, 0))

    return pl.pallas_call(
        functools.partial(local_kernel, heads),
        grid=(length // CHUNK,),
        in_specs=[
            chunk(keys),
            chunk(keys),
            chunk(vals),
            pl.BlockSpec((1, keys), lambda i: (0, 0)),
            chunk(heads),
        ],
        out_specs=[
            chunk(vals),
            chunk(keys),
            pl.BlockSpec((VAL_DIM + 16, keys), lambda i: (0, 0)),
        ],
        out_shape=[
            jax.ShapeDtypeStruct((length, vals), jnp.float32),
            jax.ShapeDtypeStruct((length, keys), jnp.bfloat16),
            jax.ShapeDtypeStruct((VAL_DIM + 16, keys), jnp.bfloat16),
        ],
        scratch_shapes=[
            pltpu.VMEM((heads, vals, KEY_DIM), jnp.float32),
            pltpu.VMEM((1, keys), jnp.float32),
        ],
        cost_estimate=pl.CostEstimate(
            flops=10_000_000_000, bytes_accessed=6_000_000, transcendentals=3_000_000
        ),
        name="local_recurrence",
    )(query, forget, values, gap.reshape(1, keys), extra)


def gate_kernel(heads, places, place_ref, rec_ref, qdec_ref, carry_ref, gain_ref, gate_ref, out_ref, held):
    rows, vals = rec_ref.shape

    @pl.when(pl.program_id(0) == 0)
    def _():
        place = place_ref[0]
        total = jnp.zeros((VAL_DIM, heads * KEY_DIM), jnp.float32)
        for i in range(places):
            decay = carry_ref[i, VAL_DIM:, :].astype(jnp.float32)[:1]
            joined = total * decay + carry_ref[i, :VAL_DIM, :].astype(jnp.float32)
            total = jnp.where(i < place, joined, total)
        lane_head = lax.broadcasted_iota(jnp.int32, total.shape, 1) // KEY_DIM
        for h in range(heads):
            held[h * VAL_DIM : (h + 1) * VAL_DIM, :] = jnp.where(lane_head == h, total, 0.0).astype(
                jnp.bfloat16
            )

    rec = rec_ref[...] + lax.dot_general(
        qdec_ref[...], held[...], NT, preferred_element_type=jnp.float32
    )
    at = lax.broadcasted_iota(jnp.int32, (vals, vals), 0) // VAL_DIM
    of = lax.broadcasted_iota(jnp.int32, (vals, vals), 1) // VAL_DIM
    average = jnp.where(at == of, 1.0 / VAL_DIM, 0.0).astype(jnp.bfloat16)
    square = rec * rec
    high = square.astype(jnp.bfloat16)
    low = (square - high.astype(jnp.float32)).astype(jnp.bfloat16)
    mean = jnp.dot(high, average, preferred_element_type=jnp.float32) + jnp.dot(
        low, average, preferred_element_type=jnp.float32
    )
    gate = gate_ref[...].astype(jnp.float32)
    gate = gate / (1.0 + jnp.exp(-gate))
    out_ref[...] = (rec * lax.rsqrt(mean + epsilon) * gain_ref[...] * gate).astype(jnp.bfloat16)


def gated_output(rec, qdec, carries, gain, gate):
    length, vals = rec.shape
    keys = qdec.shape[1]
    heads = keys // KEY_DIM
    rows = 2 * CHUNK

    def chunk(width):
        return pl.BlockSpec((rows, width), lambda i: (i, 0))

    return pl.pallas_call(
        functools.partial(gate_kernel, heads, carries.shape[0]),
        grid=(length // rows,),
        in_specs=[
            pl.BlockSpec(memory_space=pltpu.SMEM),
            chunk(vals),
            chunk(keys),
            pl.BlockSpec(carries.shape, lambda i: (0, 0, 0)),
            pl.BlockSpec((1, vals), lambda i: (0, 0)),
            chunk(vals),
        ],
        out_specs=chunk(vals),
        out_shape=jax.ShapeDtypeStruct((length, vals), jnp.bfloat16),
        scratch_shapes=[pltpu.VMEM((vals, keys), jnp.bfloat16)],
        cost_estimate=pl.CostEstimate(
            flops=2_000_000_000, bytes_accessed=3_000_000, transcendentals=1_000_000
        ),
        name="gated_output",
    )(lax.axis_index("ep").reshape(1), rec, qdec, carries, gain.reshape(1, vals), gate)


def norm_rows(tokens, row_gain):
    tokens_float = tokens.astype(jnp.float32)
    factor = lax.rsqrt(jnp.mean(tokens_float * tokens_float, axis=-1, keepdims=True) + epsilon)
    return (tokens_float * factor * row_gain).astype(jnp.bfloat16)


def slot_positions(blocks, experts_all):
    flattened = blocks.reshape(blocks.shape[0], -1)
    onehot = (flattened[..., None] == jnp.arange(experts_all, dtype=jnp.int32)).astype(jnp.int32)
    earlier = jnp.cumsum(onehot, axis=1) - onehot
    return jnp.sum(earlier * onehot, axis=-1).reshape(blocks.shape)


def fill_slots(rows_in, blocks, slot_ids, experts_all, capacity):
    groups = blocks.shape[0]
    sub_rows = blocks.shape[1]
    group_ids = jnp.arange(groups, dtype=jnp.int32)[:, None, None]
    target = (group_ids * experts_all + blocks) * capacity + slot_ids
    sources = jnp.broadcast_to(
        jnp.arange(sub_rows, dtype=jnp.int32)[None, :, None] + group_ids * sub_rows, blocks.shape
    )
    lookup = (
        jnp.full((groups * experts_all * capacity,), -1, jnp.int32)
        .at[target.reshape(-1)]
        .set(sources.reshape(-1))
    )
    gathered = rows_in.reshape(groups * sub_rows, -1)[jnp.maximum(lookup, 0)]
    filled = jnp.where((lookup >= 0)[:, None], gathered, jnp.zeros((), gathered.dtype))
    return filled.reshape(groups, experts_all, capacity, -1)


def general(
    query_preactivation,
    forget_preactivation,
    value_input_rows,
    output_gate_preactivation,
    forget_floor_gap,
    extra_log_forget,
    head_output_gain,
    mixer_output_weight,
    second_batch_tokens,
    feedforward_norm_gain,
    chosen_expert_index,
    chosen_expert_weight,
    expert_gate_weight,
    expert_up_weight,
    expert_down_weight,
):
    local_experts = expert_gate_weight.shape[0]
    places = lax.axis_size("ep")
    experts_all = local_experts * places
    groups = lax.axis_size("tp")
    width = second_batch_tokens.shape[1]
    sub_rows = second_batch_tokens.shape[0] // groups
    capacity = max(2, sub_rows * TOPK * 5 // (4 * experts_all))
    place = lax.axis_index("ep")
    position = lax.axis_index("tp")
    pairs = groups // 2
    side = lax.rem(position, 2)

    all_routes = chosen_expert_index.reshape(pairs, 2, sub_rows, TOPK)
    routes = lax.dynamic_index_in_dim(all_routes, side, 1, False)
    all_tokens = second_batch_tokens.reshape(pairs, 2, sub_rows, width)
    tokens = lax.dynamic_index_in_dim(all_tokens, side, 1, False)
    slots = slot_positions(routes, experts_all)
    outgoing = fill_slots(
        norm_rows(tokens, feedforward_norm_gain), routes, slots, experts_all, capacity
    )
    outgoing, query_preactivation = lax.optimization_barrier((outgoing, query_preactivation))
    outgoing = outgoing.reshape(pairs, places, local_experts, capacity, width)
    arrived = []
    for step in range(places):
        block = lax.dynamic_index_in_dim(outgoing, place ^ step, 1, False)
        if step:
            block = lax.ppermute(block, "ep", [(i, i ^ step) for i in range(places)])
        arrived.append(block)
    partners = [(i, i ^ 1) for i in range(groups)]
    shape = (pairs, places, local_experts, capacity, width)
    others = [lax.ppermute(block, "tp", partners) for block in arrived]
    own_side = jnp.stack(arrived, axis=1)
    other_side = jnp.stack(others, axis=1)

    recurrent, query_decayed, carry = local_recurrence(
        query_preactivation,
        forget_preactivation,
        value_input_rows,
        forget_floor_gap,
        extra_log_forget,
    )
    carries = lax.all_gather(carry, "ep")
    mixed = gated_output(
        recurrent, query_decayed, carries, head_output_gain, output_gate_preactivation
    )
    mixed_all = lax.all_gather(mixed, "tp", axis=1, tiled=True)

    def experts(rows):
        gate_part = jnp.einsum(
            "tsecd,edf->tsecf", rows, expert_gate_weight, preferred_element_type=jnp.float32
        )
        up_part = jnp.einsum(
            "tsecd,edf->tsecf", rows, expert_up_weight, preferred_element_type=jnp.float32
        )
        hidden = (jax.nn.silu(gate_part) * up_part).astype(jnp.bfloat16)
        product = jnp.einsum(
            "tsecf,efd->tsecd", hidden, expert_down_weight, preferred_element_type=jnp.float32
        )
        return product.astype(jnp.bfloat16)

    other_side, mixed = lax.optimization_barrier((other_side, mixed))
    for_partner = experts(other_side)
    own_side, for_partner = lax.optimization_barrier((own_side, for_partner))
    from_partner = lax.ppermute(for_partner, "tp", partners)
    product = experts(own_side).astype(jnp.float32) + from_partner.astype(jnp.float32)
    product, mixed_all = lax.optimization_barrier((product.astype(jnp.bfloat16), mixed_all))
    to_return = lax.psum_scatter(
        product,
        "tp",
        scatter_dimension=0,
        tiled=True,
        axis_index_groups=[list(range(c, groups, 2)) for c in range(2)],
    )
    to_return = to_return.reshape(shape[1:])
    mixer_output_first = jnp.dot(
        mixed_all, mixer_output_weight, preferred_element_type=jnp.float32
    ).astype(jnp.bfloat16)
    returned = []
    for step in range(places):
        block = to_return[step]
        if step:
            block = lax.ppermute(block, "ep", [(i, i ^ step) for i in range(places)])
        returned.append(block)
    results = jnp.concatenate(returned, axis=0).reshape(experts_all * capacity, width)
    own_routes = lax.dynamic_index_in_dim(routes, position // 2, 0, False)
    own_slots = lax.dynamic_index_in_dim(slots, position // 2, 0, False)
    own_weights = lax.dynamic_slice_in_dim(chosen_expert_weight, position * sub_rows, sub_rows, 0)
    holder = (own_routes // local_experts) ^ place
    flat_index = (holder * local_experts + own_routes % local_experts) * capacity + own_slots
    combined = jnp.zeros((sub_rows, width), jnp.float32)
    for ranked in range(TOPK):
        combined = (
            combined
            + results[flat_index[:, ranked]].astype(jnp.float32)
            * own_weights[:, ranked : ranked + 1]
        )
    return (mixer_output_first, combined.astype(jnp.bfloat16))


MESH = pl.DeviceIdType.MESH
LANES = 128
ROW_CHUNKS = 4


def fused_kernel(
    idx_ref, weight_ref, norm_gain_ref, gap_ref, extra_ref, head_gain_ref,
    tok_hbm, q_hbm, f_hbm, v_hbm, g_hbm, wo_hbm, wg_hbm, wu_hbm, wd_hbm,
    out_ref, moe_ref,
    tok, q, f, v, gate, wo, wgu, wd,
    send_rows, rows, hidden, pair_out, pair_in, psum, from_end, from_mate, from_inner,
    result_out, results, combined, moe_buf,
    state, base, carries, rec, qdec, held_state, mixed_all, out_acc,
    load_sem, disp_send, disp_recv, dfwd_send, dfwd_recv, pair_send, pair_recv,
    end_send, end_recv, mate_send, mate_recv, inner_send, inner_recv,
    ret_send, ret_recv, swap_send, swap_recv, carry_send, carry_recv,
    own_send, own_recv, right_send, left_send, ag_recv, agf_send, agf_recv,
):
    f32, bf16 = jnp.float32, jnp.bfloat16
    ep = lax.axis_index("ep")
    tp = lax.axis_index("tp")
    z, c = tp // 2, tp % 2
    last_z = mixed_all.shape[0] - 1
    oc = 1 - c
    mate = z + 1 - 2 * (z % 2)
    is_end = (z == 0) | (z == last_z)
    is_inner = (z > 0) & (z < last_z)
    places = rows.shape[0]
    steps = places
    pairs = mixed_all.shape[0]
    two = idx_ref.shape[1] // pairs
    sub = two // 2
    width = tok.shape[1]
    hw = width // 2
    rows_all = rows.shape[1]
    cp = rows_all // pairs
    cap = cp // 2
    length, keys = q.shape
    vals = v.shape[1]
    heads = keys // KEY_DIM
    blocks_f = wgu.shape[0]
    vc = vals
    ep_peer = [{"ep": ep ^ s} for s in range(places)]
    z_peer = [{"tp": (z ^ x) * 2 + c} for x in range(pairs)]
    partner = {"tp": z * 2 + oc}
    mate_dev = {"tp": mate * 2 + c}
    across_dev = {"tp": (pairs - 1 - z) * 2 + c}

    def half(i):
        return pl.ds(pl.multiple_of(i * hw, LANES), hw)

    def vcols(i):
        return pl.ds(pl.multiple_of(i * vc, LANES), vc)

    def zrows(d, n=1):
        return pl.ds(pl.multiple_of(d * cp, 16), n * cp)

    def remote(src, dst, ssem, rsem, dev):
        return pltpu.make_async_remote_copy(
            src_ref=src, dst_ref=dst, send_sem=ssem, recv_sem=rsem, device_id=dev, device_id_type=MESH
        )

    loads = {}

    def load(name, src, dst):
        copy = pltpu.make_async_copy(src, dst, load_sem.at[len(loads)])
        copy.start()
        loads[name] = copy

    for g in range(pairs):
        part = pl.ds(g * two, two)
        load(("tok", g), tok_hbm.at[part], tok.at[part])
    for j in range(blocks_f):
        cols = pl.ds(j * LANES, LANES)
        load(("wg", j), wg_hbm.at[0, :, cols], wgu.at[j, :, pl.ds(0, LANES)])
        load(("wu", j), wu_hbm.at[0, :, cols], wgu.at[j, :, pl.ds(LANES, LANES)])
    load("wd", wd_hbm.at[0], wd)
    load("q", q_hbm, q)
    load("f", f_hbm, f)
    load("v", v_hbm, v)
    load("gate", g_hbm, gate)
    load("wo", wo_hbm, wo)

    barrier = pltpu.get_barrier_semaphore()
    greet = ep_peer[1:] + z_peer[1:] + [partner]
    for dev in greet:
        pl.semaphore_signal(barrier, inc=1, device_id=dev, device_id_type=MESH)

    tri_a = lax.broadcasted_iota(jnp.int32, (two, two), 0)
    tri_b = lax.broadcasted_iota(jnp.int32, (two, two), 1)
    earlier = jnp.where((tri_a < tri_b) & (tri_a // sub == tri_b // sub), 1.0, 0.0).astype(bf16)
    lane_side = lax.broadcasted_iota(jnp.int32, (8, two), 1) // sub
    slot_row = lax.broadcasted_iota(jnp.int32, (cp, two), 0).astype(f32)
    expert_row = ep ^ lax.broadcasted_iota(jnp.int32, (8, two), 0)

    def targets(lanes):
        first = jnp.broadcast_to(idx_ref[0:1, lanes], (8, two)) == expert_row
        second = jnp.broadcast_to(idx_ref[1:2, lanes], (8, two)) == expert_row
        match = first | second
        before = jnp.dot(jnp.where(match, 1.0, 0.0).astype(bf16), earlier, preferred_element_type=f32)
        where_to = jnp.where(match, before + (lane_side * cap).astype(f32), -1.0)
        return where_to, first, second

    def dispatch(s, g):
        return remote(
            send_rows.at[s - 1, zrows(g)], rows.at[s, zrows(g), half(c)],
            disp_send.at[s - 1, g], disp_recv.at[s - 1, g], ep_peer[s],
        )

    def dispatch_forward(s, g, side):
        here = rows.at[s, zrows(g), half(side)]
        return remote(here, here, dfwd_send.at[s - 1, g], dfwd_recv.at[s - 1, g], partner)

    for g in range(pairs):
        part = slice(g * two, (g + 1) * two)
        loads[("tok", g)].wait()
        tokens = tok[part, :].astype(f32)
        factor = lax.rsqrt(jnp.mean(tokens * tokens, axis=-1, keepdims=True) + epsilon)
        tok[part, :] = (tokens * factor * norm_gain_ref[...]).astype(bf16)
        where_to, _, _ = targets(slice(g * two, (g + 1) * two))
        onehots = [
            jnp.where(slot_row == where_to[s : s + 1, :], 1.0, 0.0).astype(bf16) for s in range(places)
        ]
        own_half = tok[part, half(c)]
        for s in range(1, places):
            send_rows[s - 1, g * cp : (g + 1) * cp, :] = jnp.dot(
                onehots[s], own_half, preferred_element_type=f32
            ).astype(bf16)
        if g == 0:
            pl.semaphore_wait(barrier, len(greet))
        for s in (1, 2):
            dispatch(s, g).start()
        rows[0, g * cp : (g + 1) * cp, :] = jnp.dot(
            onehots[0], tok[part, :], preferred_element_type=f32
        ).astype(bf16)
    for g in range(pairs):
        dispatch(3, g).start()

    def forward(s, g):
        dispatch(s, g).wait_recv()
        dispatch_forward(s, g, c).start()

    def pair_copy(s):
        return remote(pair_out.at[s], pair_in.at[s], pair_send.at[s], pair_recv.at[s], partner)

    def moe(s):
        if s:
            for g in range(pairs):
                dispatch_forward(s, g, oc).wait_recv()

        def gate_up(j, _):
            acc = jnp.dot(rows[s], wgu[j], preferred_element_type=f32)
            part, up = acc[:, :LANES], acc[:, LANES:]
            value = part / (1.0 + jnp.exp(-part)) * up
            hidden[:, pl.ds(pl.multiple_of(j * LANES, LANES), LANES)] = value.astype(bf16)
            return 0

        lax.fori_loop(0, blocks_f, gate_up, 0, unroll=True)
        tile = min(256, hw)

        def down(dst, side):
            def body(j, _):
                start = pl.multiple_of(side * hw + j * tile, LANES)
                acc = jnp.dot(hidden[...], wd[:, pl.ds(start, tile)], preferred_element_type=f32)
                dst[s, :, pl.ds(pl.multiple_of(j * tile, LANES), tile)] = acc.astype(bf16)
                return 0

            lax.fori_loop(0, hw // tile, body, 0, unroll=True)

        if s == 0:
            loads["wd"].wait()
        down(pair_out, oc)
        pair_copy(s).start()
        down(psum, c)

    far = (1 - z // 2) * 2

    def end_copy(s):
        return remote(psum.at[s, zrows(far, 2)], from_end.at[s], end_send.at[s], end_recv.at[s], mate_dev)

    def mate_copy(s):
        return remote(psum.at[s, zrows(mate)], from_mate.at[s], mate_send.at[s], mate_recv.at[s], mate_dev)

    def inner_copy(s):
        return remote(psum.at[s, zrows(far, 2)], from_inner.at[s], inner_send.at[s], inner_recv.at[s], across_dev)

    def add_into(s, at, other):
        psum[s, at, :] = (psum[s, at, :].astype(f32) + other.astype(f32)).astype(bf16)

    def stage1(s):
        pair_copy(s).wait_recv()

        def body(k, _):
            at = zrows(k)
            add_into(s, at, pair_in[s, at, :])
            return 0

        lax.fori_loop(0, pairs, body, 0)

        @pl.when(is_end)
        def _():
            end_copy(s).start()

    def stage2(s):
        end_copy(s).wait_recv()

        def body(k, _):
            add_into(s, zrows(far + k), from_end[s, zrows(k), :])
            return 0

        lax.fori_loop(0, 2, body, 0)
        inner_copy(s).start()

    def stage3(s):
        inner_copy(s).wait_recv()
        add_into(s, zrows(mate), from_inner[s, zrows(mate % 2), :])
        mate_copy(s).start()

    def inner(work):
        def run():
            @pl.when(is_inner)
            def _():
                work()

        return run

    def result_copy(s):
        return remote(
            result_out.at[s], results.at[pl.ds(s * cp, cp)], ret_send.at[s - 1], ret_recv.at[s - 1], ep_peer[s]
        )

    def stage4(s, inside):
        mate_copy(s).wait_recv()
        total = psum[s, zrows(z), :].astype(f32) + from_mate[s].astype(f32)
        here = slice(s * cp, (s + 1) * cp)

        def put(value):
            if s:
                result_out[s] = value.astype(bf16)
            else:
                results[here, :] = value.astype(bf16)

        if inside:
            total = total + from_inner[s, zrows(z % 2), :].astype(f32)
        put(total)

        if s:
            result_copy(s).start()

    def carry_copy(s):
        return remote(carries.at[0], carries.at[s], carry_send.at[s - 1], carry_recv.at[s - 1], ep_peer[s])

    def recurrence(services):
        state[...] = jnp.zeros_like(state)
        base[...] = jnp.zeros_like(base)
        n = CHUNK
        at = lax.broadcasted_iota(jnp.int32, (n, n), 0)
        of = lax.broadcasted_iota(jnp.int32, (n, n), 1)
        same = (at >= of) & (at // BLOCK_POSITIONS == of // BLOCK_POSITIONS)
        lower = jnp.where(same, 1.0, 0.0).astype(bf16)
        er = lax.broadcasted_iota(jnp.int32, (8, n), 0)
        pick_row = lax.broadcasted_iota(jnp.int32, (8, keys), 0)
        pick_head = lax.broadcasted_iota(jnp.int32, (8, keys), 1) // KEY_DIM
        pick = jnp.where((pick_row % heads == pick_head) & (pick_row < 3 * heads), 1.0, 0.0).astype(bf16)
        small = (BLOCK_POSITIONS, BLOCK_POSITIONS)
        causal = lax.broadcasted_iota(jnp.int32, small, 0) >= lax.broadcasted_iota(jnp.int32, small, 1)
        lane_head = lax.broadcasted_iota(jnp.int32, (BLOCK_POSITIONS, vals), 1) // VAL_DIM

        def chunk(i, _):
            for when, work in services.items():

                @pl.when(i == when)
                def _():
                    work()

            start = pl.multiple_of(i * n, n)
            here = pl.ds(start, n)
            qc = q[here, :].astype(f32)
            qc = qc / (1.0 + jnp.exp(-qc))
            key = gap_ref[...] / (1.0 + jnp.exp(f[here, :].astype(f32)))
            terms = jnp.zeros((8, n), f32)
            for h in range(heads):
                value = jnp.broadcast_to(extra_ref[h : h + 1, here], (8, n))
                one = value.astype(bf16).astype(f32)
                second = (value - one).astype(bf16).astype(f32)
                third = value - one - second
                terms = jnp.where(er == h, one, terms)
                terms = jnp.where(er == heads + h, second, terms)
                terms = jnp.where(er == 2 * heads + h, third, terms)
            extra = lax.dot_general(terms.astype(bf16), pick, TN, preferred_element_type=f32)
            log_forget = jnp.log(1.0 - key) + extra
            high = log_forget.astype(bf16)
            low = (log_forget - high.astype(f32)).astype(bf16)
            cumulative = jnp.dot(lower, high, preferred_element_type=f32) + jnp.dot(
                lower, low, preferred_element_type=f32
            )
            held = [state[h] for h in range(heads)]
            before = base[...]
            mid_at = BLOCK_POSITIONS // 2
            for b in range(n // BLOCK_POSITIONS):
                part = slice(b * BLOCK_POSITIONS, (b + 1) * BLOCK_POSITIONS)
                block = pl.ds(start + b * BLOCK_POSITIONS, BLOCK_POSITIONS)
                cum = cumulative[part]
                mid, last = cum[mid_at - 1 : mid_at], cum[BLOCK_POSITIONS - 1 :]
                q_part = qc[part]
                q_mid = (q_part * jnp.exp(cum - mid)).astype(bf16)
                k_mid = (key[part] * jnp.exp(mid - cum)).astype(bf16)
                qdec[block, :] = (q_part * jnp.exp(cum + before)).astype(bf16)
                decay_mid, decay_last, decay_rest = jnp.exp(mid), jnp.exp(last), jnp.exp(last - mid)
                before = before + last
                values = v[block, :]
                out = jnp.zeros((BLOCK_POSITIONS, vals), f32)
                for h in range(heads):
                    lanes = slice(h * KEY_DIM, (h + 1) * KEY_DIM)
                    across = lax.dot_general(
                        q_mid[:, lanes],
                        (held[h] * decay_mid[:, lanes]).astype(bf16),
                        NT,
                        preferred_element_type=f32,
                    )
                    scores = lax.dot_general(q_mid[:, lanes], k_mid[:, lanes], NT, preferred_element_type=f32)
                    scores = jnp.where(causal, scores, 0.0).astype(bf16)
                    within = jnp.dot(scores, values, preferred_element_type=f32)
                    out = jnp.where(lane_head == h, within + across, out)
                    update = lax.dot_general(values, k_mid[:, lanes], TN, preferred_element_type=f32)
                    held[h] = held[h] * decay_last[:, lanes] + update * decay_rest[:, lanes]
                rec[block, :] = out
            for h in range(heads):
                state[h] = held[h]
            base[...] = before
            return 0

        lax.fori_loop(0, length // n, chunk, 0)
        own = [state[h, h * VAL_DIM : (h + 1) * VAL_DIM, :] for h in range(heads)]
        carries[0, :VAL_DIM, :] = jnp.concatenate(own, axis=1).astype(bf16)
        total = jnp.exp(base[...])
        carries[0, VAL_DIM:, :] = jnp.broadcast_to(total, (16, keys)).astype(bf16)
        for s in range(1, places):
            carry_copy(s).start()

    chunk_rows = length // ROW_CHUNKS

    def rows_of(r):
        return pl.ds(r * chunk_rows, chunk_rows)

    def own_copy(r, side):
        here = mixed_all.at[z, side, rows_of(r)]
        return remote(here, here, own_send.at[r], own_recv.at[r], partner)

    def hop_right(src, r):
        here = mixed_all.at[src, c, rows_of(r)]
        to = {"tp": jnp.minimum(z + 1, last_z) * 2 + c}
        return remote(here, here, right_send.at[src, r], ag_recv.at[src, r], to)

    def hop_left(src, r):
        here = mixed_all.at[src, c, rows_of(r)]
        to = {"tp": jnp.maximum(z - 1, 0) * 2 + c}
        return remote(here, here, left_send.at[src, r], ag_recv.at[src, r], to)

    def ag_forward(src, r, side):
        here = mixed_all.at[src, side, rows_of(r)]
        return remote(here, here, agf_send.at[src, r], agf_recv.at[src, r], partner)

    def source(j, inside):
        at = (None, 2, 0, 3)[j] if inside else j
        return jnp.where(z < 2, at, last_z - at)

    def start_own(r):
        @pl.when(z < last_z)
        def _():
            hop_right(z, r).start()

        @pl.when(z > 0)
        def _():
            hop_left(z, r).start()

    def ag_step(j, inside, r):
        src = source(j, inside)
        hop_right(src, r).wait_recv()
        if inside:

            @pl.when(src < z)
            def _():
                hop_right(src, r).start()

            @pl.when(src > z)
            def _():
                hop_left(src, r).start()

        ag_forward(src, r, c).start()

    def gated():
        for s in range(1, places):
            carry_copy(s).wait_recv()
        total = jnp.zeros((VAL_DIM, keys), f32)
        for i in range(places):
            decay = carries[ep ^ i, VAL_DIM:, :].astype(f32)[:1]
            joined = total * decay + carries[ep ^ i, :VAL_DIM, :].astype(f32)
            total = jnp.where(i < ep, joined, total)
        lane_head = lax.broadcasted_iota(jnp.int32, total.shape, 1) // KEY_DIM
        for h in range(heads):
            held_state[h * VAL_DIM : (h + 1) * VAL_DIM, :] = jnp.where(lane_head == h, total, 0.0).astype(bf16)
        at = lax.broadcasted_iota(jnp.int32, (vals, vals), 0) // VAL_DIM
        of = lax.broadcasted_iota(jnp.int32, (vals, vals), 1) // VAL_DIM
        average = jnp.where(at == of, 1.0 / VAL_DIM, 0.0).astype(bf16)
        for r in range(ROW_CHUNKS):
            here = rows_of(r)
            whole = rec[here, :] + lax.dot_general(
                qdec[here, :], held_state[...], NT, preferred_element_type=f32
            )
            square = whole * whole
            high = square.astype(bf16)
            low = (square - high.astype(f32)).astype(bf16)
            mean = jnp.dot(high, average, preferred_element_type=f32) + jnp.dot(
                low, average, preferred_element_type=f32
            )
            opened = gate[here, :].astype(f32)
            opened = opened / (1.0 + jnp.exp(-opened))
            mixed = (whole * lax.rsqrt(mean + epsilon) * head_gain_ref[...] * opened).astype(bf16)
            mixed_all[z, c, here, :] = mixed

            @pl.when(is_inner)
            def _():
                start_own(r)

            own_copy(r, c).start()

    def project(j, inside, r):
        src = source(j, inside) if j else z
        if j:
            ag_forward(src, r, oc).wait_recv()
        else:
            own_copy(r, oc).wait_recv()
        here = rows_of(r)
        weight = wo[pl.ds(pl.multiple_of(src * 2 * vc, LANES), 2 * vc), :]
        both = jnp.concatenate([mixed_all[src, 0, here, :], mixed_all[src, 1, here, :]], axis=1)
        part = jnp.dot(both, weight, preferred_element_type=f32)
        if j:
            part = part + out_acc[here, :]
        if j == last_z:
            out_ref[here, :] = part.astype(bf16)
        else:
            out_acc[here, :] = part

    def swap_copy():
        return remote(
            combined.at[pl.ds(pl.multiple_of(oc * sub, 16), sub)],
            moe_buf.at[:, half(c)], swap_send.at[0], swap_recv.at[0], partner,
        )

    def swap_in():
        return remote(
            combined.at[pl.ds(pl.multiple_of(oc * sub, 16), sub)],
            moe_buf.at[:, half(oc)], swap_send.at[0], swap_recv.at[0], partner,
        )

    def combine():
        lanes = pl.ds(pl.multiple_of(z * two, LANES), two)
        where_to, first, second = targets(lanes)
        weight = jnp.where(first, jnp.broadcast_to(weight_ref[0:1, lanes], (8, two)), 0.0) + jnp.where(
            second, jnp.broadcast_to(weight_ref[1:2, lanes], (8, two)), 0.0
        )
        high = weight.astype(bf16).astype(f32)
        low = weight - high
        picks = [slot_row == where_to[s : s + 1, :] for s in range(places)]
        coarse = jnp.concatenate(
            [jnp.where(picks[s], high[s : s + 1, :], 0.0).astype(bf16) for s in range(places)], axis=0
        )
        fine = jnp.concatenate(
            [jnp.where(picks[s], low[s : s + 1, :], 0.0).astype(bf16) for s in range(places)], axis=0
        )
        for s in range(1, places):
            result_copy(s).wait_recv()
        total = lax.dot_general(coarse, results[...], TN, preferred_element_type=f32) + lax.dot_general(
            fine, results[...], TN, preferred_element_type=f32
        )
        combined[...] = total.astype(bf16)
        swap_copy().start()

    def finish():
        moe_buf[:, half(c)] = combined[pl.ds(pl.multiple_of(c * sub, 16), sub), :]
        swap_in().wait_recv()
        moe_ref[...] = moe_buf[...]

    chunks = range(ROW_CHUNKS)
    for j in range(blocks_f):
        loads[("wg", j)].wait()
        loads[("wu", j)].wait()
    moe(0)
    for name in ("q", "f", "v"):
        loads[name].wait()

    def take(s):
        for g in range(pairs):
            forward(s, g)

    recurrence({1: lambda: stage1(0), 6: inner(lambda: stage2(0))})
    take(1)
    take(2)
    moe(1)
    loads["gate"].wait()
    gated()
    stage1(1)
    inner(lambda: stage3(0))()
    moe(2)
    take(3)
    stage1(2)
    moe(3)
    loads["wo"].wait()
    stage1(3)

    @pl.when(is_end)
    def _():
        for r in chunks:
            start_own(r)
        for s in range(places):
            mate_copy(s).start()
        for r in chunks:
            project(0, False, r)
            ag_step(1, False, r)
        stage4(0, False)
        for r in chunks:
            ag_step(2, False, r)
            project(1, False, r)
        stage4(1, False)
        stage4(2, False)
        for r in chunks:
            project(2, False, r)
        for r in (0, 1):
            ag_step(3, False, r)
        stage4(3, False)
        for r in (2, 3):
            ag_step(3, False, r)
        for r in chunks:
            project(3, False, r)

    @pl.when(is_inner)
    def _():
        stage2(1)
        for r in chunks:
            project(0, True, r)
            ag_step(1, True, r)
        stage2(2)
        stage3(1)
        for r in chunks:
            project(1, True, r)
        stage2(3)
        ag_step(2, True, 0)
        stage3(2)
        ag_step(2, True, 1)
        ag_step(3, True, 0)
        ag_step(2, True, 2)
        ag_step(3, True, 1)
        stage3(3)
        ag_step(2, True, 3)
        ag_step(3, True, 2)
        for r in chunks:
            project(2, True, r)
        ag_step(3, True, 3)
        for s in range(places):
            stage4(s, True)
        for r in chunks:
            project(3, True, r)

    combine()
    finish()

    for s in range(1, places):
        for g in range(pairs):
            dispatch(s, g).wait_send()
            dispatch_forward(s, g, c).wait_send()
        carry_copy(s).wait_send()
        result_copy(s).wait_send()
    for s in range(places):
        pair_copy(s).wait_send()
        mate_copy(s).wait_send()

        @pl.when(is_end)
        def _():
            end_copy(s).wait_send()

        @pl.when(is_inner)
        def _():
            inner_copy(s).wait_send()

    for r in chunks:
        own_copy(r, c).wait_send()
        for src in range(pairs):

            @pl.when((src <= z) & (z < last_z))
            def _():
                hop_right(src, r).wait_send()

            @pl.when((src >= z) & (z > 0))
            def _():
                hop_left(src, r).wait_send()

            @pl.when(src != z)
            def _():
                ag_forward(src, r, c).wait_send()

    swap_copy().wait_send()


def on_device(*arrays):
    (
        query, forget, values, gate, gap, extra, head_gain, out_weight,
        tokens, norm_gain, index, weight, gate_weight, up_weight, down_weight,
    ) = arrays
    places, groups = lax.axis_size("ep"), lax.axis_size("tp")
    pairs = groups // 2
    length, keys = query.shape
    vals = values.shape[1]
    count, width = tokens.shape
    hidden = gate_weight.shape[2]
    sub = count // groups
    experts_all = gate_weight.shape[0] * places
    capacity = max(2, sub * TOPK * 5 // (4 * experts_all))
    fits = (
        places == 4
        and groups == 8
        and gate_weight.shape[0] == 1
        and 2 * sub == LANES
        and capacity % 8 == 0
        and capacity <= sub
        and vals == LANES
        and keys == 2 * KEY_DIM
        and length % (ROW_CHUNKS * CHUNK) == 0
        and hidden % LANES == 0
        and width % 512 == 0
    )
    if not fits:
        return general(*arrays)
    heads = keys // KEY_DIM
    cp = 2 * capacity
    rows_all = pairs * cp
    hw = width // 2
    features = out_weight.shape[1]
    bf16, f32 = jnp.bfloat16, jnp.float32
    vmem = pl.BlockSpec(memory_space=pltpu.VMEM)
    anywhere = pl.BlockSpec(memory_space=pl.ANY)
    dma = pltpu.SemaphoreType.DMA
    scratch = [
        pltpu.VMEM((count, width), bf16),
        pltpu.VMEM((length, keys), bf16),
        pltpu.VMEM((length, keys), bf16),
        pltpu.VMEM((length, vals), bf16),
        pltpu.VMEM((length, vals), bf16),
        pltpu.VMEM(out_weight.shape, bf16),
        pltpu.VMEM((hidden // LANES, width, 2 * LANES), bf16),
        pltpu.VMEM((hidden, width), bf16),
        pltpu.VMEM((places - 1, rows_all, hw), bf16),
        pltpu.VMEM((places, rows_all, width), bf16),
        pltpu.VMEM((rows_all, hidden), bf16),
        pltpu.VMEM((places, rows_all, hw), bf16),
        pltpu.VMEM((places, rows_all, hw), bf16),
        pltpu.VMEM((places, rows_all, hw), bf16),
        pltpu.VMEM((places, 2 * cp, hw), bf16),
        pltpu.VMEM((places, cp, hw), bf16),
        pltpu.VMEM((places, 2 * cp, hw), bf16),
        pltpu.VMEM((places, cp, hw), bf16),
        pltpu.VMEM((places * cp, hw), bf16),
        pltpu.VMEM((2 * sub, hw), bf16),
        pltpu.VMEM((sub, width), bf16),
        pltpu.VMEM((heads, vals, KEY_DIM), f32),
        pltpu.VMEM((1, keys), f32),
        pltpu.VMEM((places, VAL_DIM + 16, keys), bf16),
        pltpu.VMEM((length, vals), f32),
        pltpu.VMEM((length, keys), bf16),
        pltpu.VMEM((vals, keys), bf16),
        pltpu.VMEM((pairs, 2, length, vals), bf16),
        pltpu.VMEM((length, features), f32),
    ]
    n_loads = pairs + 2 * (hidden // LANES) + 6
    peers = places - 1
    sems = [dma((n_loads,))]
    sems += [dma((peers, pairs))] * 4 + [dma((places,))] * 8 + [dma((peers,))] * 2 + [dma((1,))] * 2
    sems += [dma((peers,))] * 2 + [dma((ROW_CHUNKS,))] * 2 + [dma((pairs, ROW_CHUNKS))] * 5
    return pl.pallas_call(
        fused_kernel,
        in_specs=[vmem] * 6 + [anywhere] * 9,
        out_specs=[vmem, vmem],
        out_shape=[
            jax.ShapeDtypeStruct((length, features), bf16),
            jax.ShapeDtypeStruct((sub, width), bf16),
        ],
        scratch_shapes=scratch + sems,
        compiler_params=pltpu.CompilerParams(
            collective_id=0, has_side_effects=True, vmem_limit_bytes=64 * 1024 * 1024 - 65536
        ),
        name="fused_layer",
    )(
        index.T, weight.T, norm_gain.reshape(1, width), gap.reshape(1, keys), extra.T,
        head_gain.reshape(1, vals), tokens, query, forget, values, gate, out_weight,
        gate_weight, up_weight, down_weight,
    )


def solution(mesh):
    placed = (
        P("ep", "tp"),
        P("ep", "tp"),
        P("ep", "tp"),
        P("ep", "tp"),
        P("tp"),
        P("ep", "tp"),
        P("tp"),
        P(None, "tp"),
        P("ep", None),
        P(),
        P("ep", None),
        P("ep", None),
        P("ep", None, "tp"),
        P("ep", None, "tp"),
        P("ep", "tp", None),
    )
    return jax.shard_map(
        on_device,
        mesh=mesh,
        in_specs=placed,
        out_specs=(P("ep", "tp"), P(("ep", "tp"), None)),
        check_vma=False,
    )
```

```python
import functools

import jax
import jax.numpy as jnp
from jax import lax
from jax.experimental import pallas as pl
from jax.experimental.pallas import tpu as pltpu
from jax.sharding import PartitionSpec as P

KEY_DIM = 128
VAL_DIM = 64
BLOCK_POSITIONS = 64
TOPK = 2


epsilon = 1e-06


CHUNK = 256
NT = (((1,), (1,)), ((), ()))
TN = (((0,), (0,)), ((), ()))


def local_kernel(heads, q_ref, f_ref, v_ref, gap_ref, extra_ref, rec_ref, qdec_ref, carry_ref, state, base):
    step = pl.program_id(0)

    @pl.when(step == 0)
    def _():
        state[...] = jnp.zeros_like(state)
        base[...] = jnp.zeros_like(base)

    rows, vals = v_ref.shape
    q = q_ref[...].astype(jnp.float32)
    q = q / (1.0 + jnp.exp(-q))
    key = gap_ref[...] / (1.0 + jnp.exp(f_ref[...].astype(jnp.float32)))
    extra = extra_ref[...]
    log_forget = jnp.log(1.0 - key) + jnp.concatenate(
        [jnp.broadcast_to(extra[:, h : h + 1], (rows, KEY_DIM)) for h in range(heads)], axis=1
    )
    at = lax.broadcasted_iota(jnp.int32, (rows, rows), 0)
    of = lax.broadcasted_iota(jnp.int32, (rows, rows), 1)
    lower = jnp.where((at >= of) & (at // BLOCK_POSITIONS == of // BLOCK_POSITIONS), 1.0, 0.0)
    lower = lower.astype(jnp.bfloat16)
    high = log_forget.astype(jnp.bfloat16)
    low = (log_forget - high.astype(jnp.float32)).astype(jnp.bfloat16)
    cumulative = jnp.dot(lower, high, preferred_element_type=jnp.float32) + jnp.dot(
        lower, low, preferred_element_type=jnp.float32
    )
    causal = lax.broadcasted_iota(
        jnp.int32, (BLOCK_POSITIONS, BLOCK_POSITIONS), 0
    ) >= lax.broadcasted_iota(jnp.int32, (BLOCK_POSITIONS, BLOCK_POSITIONS), 1)
    lane_head = lax.broadcasted_iota(jnp.int32, (BLOCK_POSITIONS, vals), 1) // VAL_DIM
    held = [state[h] for h in range(heads)]
    before = base[...]
    half = BLOCK_POSITIONS // 2
    for b in range(rows // BLOCK_POSITIONS):
        part = slice(b * BLOCK_POSITIONS, (b + 1) * BLOCK_POSITIONS)
        cum = cumulative[part]
        mid, last = cum[half - 1 : half], cum[BLOCK_POSITIONS - 1 :]
        q_part = q[part]
        q_mid = (q_part * jnp.exp(cum - mid)).astype(jnp.bfloat16)
        k_mid = (key[part] * jnp.exp(mid - cum)).astype(jnp.bfloat16)
        qdec_ref[part, :] = (q_part * jnp.exp(cum + before)).astype(jnp.bfloat16)
        decay_mid, decay_last, decay_rest = jnp.exp(mid), jnp.exp(last), jnp.exp(last - mid)
        before = before + last
        values = v_ref[part, :]
        out = jnp.zeros((BLOCK_POSITIONS, vals), jnp.float32)
        for h in range(heads):
            lanes = slice(h * KEY_DIM, (h + 1) * KEY_DIM)
            across = lax.dot_general(
                q_mid[:, lanes],
                (held[h] * decay_mid[:, lanes]).astype(jnp.bfloat16),
                NT,
                preferred_element_type=jnp.float32,
            )
            scores = lax.dot_general(
                q_mid[:, lanes], k_mid[:, lanes], NT, preferred_element_type=jnp.float32
            )
            scores = jnp.where(causal, scores, 0.0).astype(jnp.bfloat16)
            within = jnp.dot(scores, values, preferred_element_type=jnp.float32)
            out = jnp.where(lane_head == h, within + across, out)
            update = lax.dot_general(
                values, k_mid[:, lanes], TN, preferred_element_type=jnp.float32
            )
            held[h] = held[h] * decay_last[:, lanes] + update * decay_rest[:, lanes]
        rec_ref[part, :] = out
    for h in range(heads):
        state[h] = held[h]
    base[...] = before

    @pl.when(step == pl.num_programs(0) - 1)
    def _():
        own = [held[h][h * VAL_DIM : (h + 1) * VAL_DIM] for h in range(heads)]
        carry_ref[:VAL_DIM, :] = jnp.concatenate(own, axis=1).astype(jnp.bfloat16)
        total = jnp.exp(before)
        carry_ref[VAL_DIM:, :] = jnp.broadcast_to(total, (16, total.shape[1])).astype(jnp.bfloat16)


def local_recurrence(query, forget, values, gap, extra):
    length, keys = query.shape
    heads, vals = keys // KEY_DIM, values.shape[1]

    def chunk(width):
        return pl.BlockSpec((CHUNK, width), lambda i: (i, 0))

    return pl.pallas_call(
        functools.partial(local_kernel, heads),
        grid=(length // CHUNK,),
        in_specs=[
            chunk(keys),
            chunk(keys),
            chunk(vals),
            pl.BlockSpec((1, keys), lambda i: (0, 0)),
            chunk(heads),
        ],
        out_specs=[
            chunk(vals),
            chunk(keys),
            pl.BlockSpec((VAL_DIM + 16, keys), lambda i: (0, 0)),
        ],
        out_shape=[
            jax.ShapeDtypeStruct((length, vals), jnp.float32),
            jax.ShapeDtypeStruct((length, keys), jnp.bfloat16),
            jax.ShapeDtypeStruct((VAL_DIM + 16, keys), jnp.bfloat16),
        ],
        scratch_shapes=[
            pltpu.VMEM((heads, vals, KEY_DIM), jnp.float32),
            pltpu.VMEM((1, keys), jnp.float32),
        ],
        cost_estimate=pl.CostEstimate(
            flops=10_000_000_000, bytes_accessed=6_000_000, transcendentals=3_000_000
        ),
        name="local_recurrence",
    )(query, forget, values, gap.reshape(1, keys), extra)


def gate_kernel(heads, places, place_ref, rec_ref, qdec_ref, carry_ref, gain_ref, gate_ref, out_ref, held):
    rows, vals = rec_ref.shape

    @pl.when(pl.program_id(0) == 0)
    def _():
        place = place_ref[0]
        total = jnp.zeros((VAL_DIM, heads * KEY_DIM), jnp.float32)
        for i in range(places):
            decay = carry_ref[i, VAL_DIM:, :].astype(jnp.float32)[:1]
            joined = total * decay + carry_ref[i, :VAL_DIM, :].astype(jnp.float32)
            total = jnp.where(i < place, joined, total)
        lane_head = lax.broadcasted_iota(jnp.int32, total.shape, 1) // KEY_DIM
        for h in range(heads):
            held[h * VAL_DIM : (h + 1) * VAL_DIM, :] = jnp.where(lane_head == h, total, 0.0).astype(
                jnp.bfloat16
            )

    rec = rec_ref[...] + lax.dot_general(
        qdec_ref[...], held[...], NT, preferred_element_type=jnp.float32
    )
    at = lax.broadcasted_iota(jnp.int32, (vals, vals), 0) // VAL_DIM
    of = lax.broadcasted_iota(jnp.int32, (vals, vals), 1) // VAL_DIM
    average = jnp.where(at == of, 1.0 / VAL_DIM, 0.0).astype(jnp.bfloat16)
    square = rec * rec
    high = square.astype(jnp.bfloat16)
    low = (square - high.astype(jnp.float32)).astype(jnp.bfloat16)
    mean = jnp.dot(high, average, preferred_element_type=jnp.float32) + jnp.dot(
        low, average, preferred_element_type=jnp.float32
    )
    gate = gate_ref[...].astype(jnp.float32)
    gate = gate / (1.0 + jnp.exp(-gate))
    out_ref[...] = (rec * lax.rsqrt(mean + epsilon) * gain_ref[...] * gate).astype(jnp.bfloat16)


def gated_output(rec, qdec, carries, gain, gate):
    length, vals = rec.shape
    keys = qdec.shape[1]
    heads = keys // KEY_DIM
    rows = 2 * CHUNK

    def chunk(width):
        return pl.BlockSpec((rows, width), lambda i: (i, 0))

    return pl.pallas_call(
        functools.partial(gate_kernel, heads, carries.shape[0]),
        grid=(length // rows,),
        in_specs=[
            pl.BlockSpec(memory_space=pltpu.SMEM),
            chunk(vals),
            chunk(keys),
            pl.BlockSpec(carries.shape, lambda i: (0, 0, 0)),
            pl.BlockSpec((1, vals), lambda i: (0, 0)),
            chunk(vals),
        ],
        out_specs=chunk(vals),
        out_shape=jax.ShapeDtypeStruct((length, vals), jnp.bfloat16),
        scratch_shapes=[pltpu.VMEM((vals, keys), jnp.bfloat16)],
        cost_estimate=pl.CostEstimate(
            flops=2_000_000_000, bytes_accessed=3_000_000, transcendentals=1_000_000
        ),
        name="gated_output",
    )(lax.axis_index("ep").reshape(1), rec, qdec, carries, gain.reshape(1, vals), gate)


def norm_rows(tokens, row_gain):
    tokens_float = tokens.astype(jnp.float32)
    factor = lax.rsqrt(jnp.mean(tokens_float * tokens_float, axis=-1, keepdims=True) + epsilon)
    return (tokens_float * factor * row_gain).astype(jnp.bfloat16)


def slot_positions(blocks, experts_all):
    flattened = blocks.reshape(blocks.shape[0], -1)
    onehot = (flattened[..., None] == jnp.arange(experts_all, dtype=jnp.int32)).astype(jnp.int32)
    earlier = jnp.cumsum(onehot, axis=1) - onehot
    return jnp.sum(earlier * onehot, axis=-1).reshape(blocks.shape)


def fill_slots(rows_in, blocks, slot_ids, experts_all, capacity):
    groups = blocks.shape[0]
    sub_rows = blocks.shape[1]
    group_ids = jnp.arange(groups, dtype=jnp.int32)[:, None, None]
    target = (group_ids * experts_all + blocks) * capacity + slot_ids
    sources = jnp.broadcast_to(
        jnp.arange(sub_rows, dtype=jnp.int32)[None, :, None] + group_ids * sub_rows, blocks.shape
    )
    lookup = (
        jnp.full((groups * experts_all * capacity,), -1, jnp.int32)
        .at[target.reshape(-1)]
        .set(sources.reshape(-1))
    )
    gathered = rows_in.reshape(groups * sub_rows, -1)[jnp.maximum(lookup, 0)]
    filled = jnp.where((lookup >= 0)[:, None], gathered, jnp.zeros((), gathered.dtype))
    return filled.reshape(groups, experts_all, capacity, -1)


def general(
    query_preactivation,
    forget_preactivation,
    value_input_rows,
    output_gate_preactivation,
    forget_floor_gap,
    extra_log_forget,
    head_output_gain,
    mixer_output_weight,
    second_batch_tokens,
    feedforward_norm_gain,
    chosen_expert_index,
    chosen_expert_weight,
    expert_gate_weight,
    expert_up_weight,
    expert_down_weight,
):
    local_experts = expert_gate_weight.shape[0]
    places = lax.axis_size("ep")
    experts_all = local_experts * places
    groups = lax.axis_size("tp")
    width = second_batch_tokens.shape[1]
    sub_rows = second_batch_tokens.shape[0] // groups
    capacity = max(2, sub_rows * TOPK * 5 // (4 * experts_all))
    place = lax.axis_index("ep")
    position = lax.axis_index("tp")
    pairs = groups // 2
    side = lax.rem(position, 2)

    all_routes = chosen_expert_index.reshape(pairs, 2, sub_rows, TOPK)
    routes = lax.dynamic_index_in_dim(all_routes, side, 1, False)
    all_tokens = second_batch_tokens.reshape(pairs, 2, sub_rows, width)
    tokens = lax.dynamic_index_in_dim(all_tokens, side, 1, False)
    slots = slot_positions(routes, experts_all)
    outgoing = fill_slots(
        norm_rows(tokens, feedforward_norm_gain), routes, slots, experts_all, capacity
    )
    outgoing, query_preactivation = lax.optimization_barrier((outgoing, query_preactivation))
    outgoing = outgoing.reshape(pairs, places, local_experts, capacity, width)
    arrived = []
    for step in range(places):
        block = lax.dynamic_index_in_dim(outgoing, place ^ step, 1, False)
        if step:
            block = lax.ppermute(block, "ep", [(i, i ^ step) for i in range(places)])
        arrived.append(block)
    partners = [(i, i ^ 1) for i in range(groups)]
    shape = (pairs, places, local_experts, capacity, width)
    others = [lax.ppermute(block, "tp", partners) for block in arrived]
    own_side = jnp.stack(arrived, axis=1)
    other_side = jnp.stack(others, axis=1)

    recurrent, query_decayed, carry = local_recurrence(
        query_preactivation,
        forget_preactivation,
        value_input_rows,
        forget_floor_gap,
        extra_log_forget,
    )
    carries = lax.all_gather(carry, "ep")
    mixed = gated_output(
        recurrent, query_decayed, carries, head_output_gain, output_gate_preactivation
    )
    mixed_all = lax.all_gather(mixed, "tp", axis=1, tiled=True)

    def experts(rows):
        gate_part = jnp.einsum(
            "tsecd,edf->tsecf", rows, expert_gate_weight, preferred_element_type=jnp.float32
        )
        up_part = jnp.einsum(
            "tsecd,edf->tsecf", rows, expert_up_weight, preferred_element_type=jnp.float32
        )
        hidden = (jax.nn.silu(gate_part) * up_part).astype(jnp.bfloat16)
        product = jnp.einsum(
            "tsecf,efd->tsecd", hidden, expert_down_weight, preferred_element_type=jnp.float32
        )
        return product.astype(jnp.bfloat16)

    other_side, mixed = lax.optimization_barrier((other_side, mixed))
    for_partner = experts(other_side)
    own_side, for_partner = lax.optimization_barrier((own_side, for_partner))
    from_partner = lax.ppermute(for_partner, "tp", partners)
    product = experts(own_side).astype(jnp.float32) + from_partner.astype(jnp.float32)
    product, mixed_all = lax.optimization_barrier((product.astype(jnp.bfloat16), mixed_all))
    to_return = lax.psum_scatter(
        product,
        "tp",
        scatter_dimension=0,
        tiled=True,
        axis_index_groups=[list(range(c, groups, 2)) for c in range(2)],
    )
    to_return = to_return.reshape(shape[1:])
    mixer_output_first = jnp.dot(
        mixed_all, mixer_output_weight, preferred_element_type=jnp.float32
    ).astype(jnp.bfloat16)
    returned = []
    for step in range(places):
        block = to_return[step]
        if step:
            block = lax.ppermute(block, "ep", [(i, i ^ step) for i in range(places)])
        returned.append(block)
    results = jnp.concatenate(returned, axis=0).reshape(experts_all * capacity, width)
    own_routes = lax.dynamic_index_in_dim(routes, position // 2, 0, False)
    own_slots = lax.dynamic_index_in_dim(slots, position // 2, 0, False)
    own_weights = lax.dynamic_slice_in_dim(chosen_expert_weight, position * sub_rows, sub_rows, 0)
    holder = (own_routes // local_experts) ^ place
    flat_index = (holder * local_experts + own_routes % local_experts) * capacity + own_slots
    combined = jnp.zeros((sub_rows, width), jnp.float32)
    for ranked in range(TOPK):
        combined = (
            combined
            + results[flat_index[:, ranked]].astype(jnp.float32)
            * own_weights[:, ranked : ranked + 1]
        )
    return (mixer_output_first, combined.astype(jnp.bfloat16))


MESH = pl.DeviceIdType.MESH
LANES = 128
ROW_CHUNKS = 4


def fused_kernel(
    idx_hbm, weight_hbm, norm_gain_hbm, gap_hbm, extra_hbm, head_gain_hbm,
    tok_hbm, q_hbm, f_hbm, v_hbm, g_hbm, wo_hbm, wg_hbm, wu_hbm, wd_hbm,
    out_ref, moe_ref,
    idx_ref, weight_ref, norm_gain_ref, gap_ref, extra_ref, head_gain_ref,
    tok, q, f, v, gate, wo, wgu, wd,
    send_rows, rows, hidden, pair_out, pair_in, psum, from_end, from_mate, from_inner,
    result_out, results, combined, moe_buf,
    state, base, carries, rec, qdec, held_state, mixed_all, out_acc, out_buf,
    load_sem, disp_send, disp_recv, dfwd_send, dfwd_recv, pair_send, pair_recv,
    end_send, end_recv, mate_send, mate_recv, inner_send, inner_recv,
    ret_send, ret_recv, swap_send, swap_recv, carry_send, carry_recv,
    own_send, own_recv, right_send, left_send, ag_recv, agf_send, agf_recv, out_sem,
):
    f32, bf16 = jnp.float32, jnp.bfloat16
    ep = lax.axis_index("ep")
    tp = lax.axis_index("tp")
    z, c = tp // 2, tp % 2
    last_z = mixed_all.shape[0] - 1
    oc = 1 - c
    mate = z + 1 - 2 * (z % 2)
    is_end = (z == 0) | (z == last_z)
    is_inner = (z > 0) & (z < last_z)
    places = rows.shape[0]
    steps = places
    pairs = mixed_all.shape[0]
    two = idx_ref.shape[1] // pairs
    sub = two // 2
    width = tok.shape[1]
    hw = width // 2
    rows_all = rows.shape[1]
    cp = rows_all // pairs
    cap = cp // 2
    length, keys = q.shape
    vals = v.shape[1]
    heads = keys // KEY_DIM
    blocks_f = wgu.shape[0]
    vc = vals
    ep_peer = [{"ep": ep ^ s} for s in range(places)]
    partner = {"tp": z * 2 + oc}
    mate_dev = {"tp": mate * 2 + c}
    across_dev = {"tp": (pairs - 1 - z) * 2 + c}

    pieces = 2
    pw = hw // pieces

    def piece(h):
        return pl.ds(h * pw, pw)

    def half(i):
        return pl.ds(pl.multiple_of(i * hw, LANES), hw)

    def vcols(i):
        return pl.ds(pl.multiple_of(i * vc, LANES), vc)

    def zrows(d, n=1):
        return pl.ds(pl.multiple_of(d * cp, 16), n * cp)

    def remote(src, dst, ssem, rsem, dev):
        return pltpu.make_async_remote_copy(
            src_ref=src, dst_ref=dst, send_sem=ssem, recv_sem=rsem, device_id=dev, device_id_type=MESH
        )

    barrier = pltpu.get_barrier_semaphore()
    for dev in ep_peer[1:] + [partner]:
        pl.semaphore_signal(barrier, inc=1, device_id=dev, device_id_type=MESH)

    @pl.when(z > 0)
    def _():
        pl.semaphore_signal(barrier, inc=1, device_id={"tp": tp - 2}, device_id_type=MESH)

    @pl.when(z < last_z)
    def _():
        pl.semaphore_signal(barrier, inc=1, device_id={"tp": tp + 2}, device_id_type=MESH)

    loads = {}

    def load(name, src, dst):
        copy = pltpu.make_async_copy(src, dst, load_sem.at[len(loads)])
        copy.start()
        loads[name] = copy

    load("idx", idx_hbm, idx_ref)
    load("norm_gain", norm_gain_hbm, norm_gain_ref)
    for g in range(pairs):
        part = pl.ds(g * two, two)
        load(("tok", g), tok_hbm.at[part], tok.at[part])
    for j in range(blocks_f):
        cols = pl.ds(j * LANES, LANES)
        load(("wg", j), wg_hbm.at[0, :, cols], wgu.at[j, :, pl.ds(0, LANES)])
        load(("wu", j), wu_hbm.at[0, :, cols], wgu.at[j, :, pl.ds(LANES, LANES)])
    load("wd", wd_hbm.at[0], wd)
    load("weight", weight_hbm, weight_ref)
    load("gap", gap_hbm, gap_ref)
    load("extra", extra_hbm, extra_ref)
    load("head_gain", head_gain_hbm, head_gain_ref)
    load("q", q_hbm, q)
    load("f", f_hbm, f)
    load("v", v_hbm, v)
    load("gate", g_hbm, gate)
    load("wo", wo_hbm, wo)

    tri_a = lax.broadcasted_iota(jnp.int32, (two, two), 0)
    tri_b = lax.broadcasted_iota(jnp.int32, (two, two), 1)
    earlier = jnp.where((tri_a < tri_b) & (tri_a // sub == tri_b // sub), 1.0, 0.0).astype(bf16)
    lane_side = lax.broadcasted_iota(jnp.int32, (8, two), 1) // sub
    slot_row = lax.broadcasted_iota(jnp.int32, (cp, two), 0).astype(f32)
    expert_row = ep ^ lax.broadcasted_iota(jnp.int32, (8, two), 0)

    def targets(lanes):
        first = jnp.broadcast_to(idx_ref[0:1, lanes], (8, two)) == expert_row
        second = jnp.broadcast_to(idx_ref[1:2, lanes], (8, two)) == expert_row
        match = first | second
        before = jnp.dot(jnp.where(match, 1.0, 0.0).astype(bf16), earlier, preferred_element_type=f32)
        where_to = jnp.where(match, before + (lane_side * cap).astype(f32), -1.0)
        return where_to, first, second

    def dispatch(s, g):
        return remote(
            send_rows.at[s - 1, zrows(g)], rows.at[s, zrows(g), half(c)],
            disp_send.at[s - 1, g], disp_recv.at[s - 1, g], ep_peer[s],
        )

    def dispatch_forward(s, g, side):
        here = rows.at[s, zrows(g), half(side)]
        return remote(here, here, dfwd_send.at[s - 1, g], dfwd_recv.at[s - 1, g], partner)

    loads["idx"].wait()
    loads["norm_gain"].wait()
    for g in range(pairs):
        part = slice(g * two, (g + 1) * two)
        loads[("tok", g)].wait()
        tokens = tok[part, :].astype(f32)
        factor = lax.rsqrt(jnp.mean(tokens * tokens, axis=-1, keepdims=True) + epsilon)
        tok[part, :] = (tokens * factor * norm_gain_ref[...]).astype(bf16)
        where_to, _, _ = targets(slice(g * two, (g + 1) * two))
        onehots = [
            jnp.where(slot_row == where_to[s : s + 1, :], 1.0, 0.0).astype(bf16) for s in range(places)
        ]
        own_half = tok[part, half(c)]
        for s in range(1, places):
            send_rows[s - 1, g * cp : (g + 1) * cp, :] = jnp.dot(
                onehots[s], own_half, preferred_element_type=f32
            ).astype(bf16)
        if g == 0:
            pl.semaphore_wait(barrier, jnp.where(is_end, places + 1, places + 2))
        for s in (1, 2):
            dispatch(s, g).start()
        rows[0, g * cp : (g + 1) * cp, :] = jnp.dot(
            onehots[0], tok[part, :], preferred_element_type=f32
        ).astype(bf16)
    for g in range(pairs):
        dispatch(3, g).start()

    def forward(s, g):
        dispatch(s, g).wait_recv()
        dispatch_forward(s, g, c).start()

    def pair_copy(s, h):
        return remote(
            pair_out.at[s, :, piece(h)], pair_in.at[s, :, piece(h)], pair_send.at[s, h], pair_recv.at[s, h], partner
        )

    def moe(s):
        if s:
            for g in range(pairs):
                dispatch_forward(s, g, oc).wait_recv()

        def gate_up(j, _):
            acc = jnp.dot(rows[s], wgu[j], preferred_element_type=f32)
            part, up = acc[:, :LANES], acc[:, LANES:]
            value = part / (1.0 + jnp.exp(-part)) * up
            hidden[:, pl.ds(pl.multiple_of(j * LANES, LANES), LANES)] = value.astype(bf16)
            return 0

        lax.fori_loop(0, blocks_f, gate_up, 0, unroll=True)
        tile = min(256, pw)

        def down(dst, side, h):
            for j in range(pw // tile):
                start = pl.multiple_of(side * hw + h * pw + j * tile, LANES)
                acc = jnp.dot(hidden[...], wd[:, pl.ds(start, tile)], preferred_element_type=f32)
                dst[s, :, h * pw + j * tile : h * pw + (j + 1) * tile] = acc.astype(bf16)

        if s == 0:
            loads["wd"].wait()
        for h in range(pieces):
            down(pair_out, oc, h)
            pair_copy(s, h).start()
        for h in range(pieces):
            down(psum, c, h)

    far = (1 - z // 2) * 2

    def end_copy(s, h):
        return remote(
            psum.at[s, zrows(far, 2), piece(h)], from_end.at[s, :, piece(h)],
            end_send.at[s, h], end_recv.at[s, h], mate_dev,
        )

    def mate_copy(s, h):
        return remote(
            psum.at[s, zrows(mate), piece(h)], from_mate.at[s, :, piece(h)],
            mate_send.at[s, h], mate_recv.at[s, h], mate_dev,
        )

    def inner_copy(s, h):
        return remote(
            psum.at[s, zrows(far, 2), piece(h)], from_inner.at[s, :, piece(h)],
            inner_send.at[s, h], inner_recv.at[s, h], across_dev,
        )

    def add_into(s, at, h, other):
        psum[s, at, piece(h)] = (psum[s, at, piece(h)].astype(f32) + other.astype(f32)).astype(bf16)

    def stage1(s):
        for h in range(pieces):
            pair_copy(s, h).wait_recv()

            def body(k, _):
                at = zrows(k)
                add_into(s, at, h, pair_in[s, at, piece(h)])
                return 0

            lax.fori_loop(0, pairs, body, 0)

            @pl.when(is_end)
            def _():
                end_copy(s, h).start()

    def stage2(s, h):
        end_copy(s, h).wait_recv()

        def body(k, _):
            add_into(s, zrows(far + k), h, from_end[s, zrows(k), piece(h)])
            return 0

        lax.fori_loop(0, 2, body, 0)
        inner_copy(s, h).start()

    def stage3(s, h):
        inner_copy(s, h).wait_recv()
        add_into(s, zrows(mate), h, from_inner[s, zrows(mate % 2), piece(h)])
        mate_copy(s, h).start()

    def inner(work):
        def run():
            @pl.when(is_inner)
            def _():
                work()

        return run

    def result_copy(s, h):
        return remote(
            result_out.at[s, :, piece(h)], results.at[pl.ds(s * cp, cp), piece(h)],
            ret_send.at[s - 1, h], ret_recv.at[s - 1, h], ep_peer[s],
        )

    def stage4(s, h, inside):
        mate_copy(s, h).wait_recv()
        total = psum[s, zrows(z), piece(h)].astype(f32) + from_mate[s, :, piece(h)].astype(f32)
        if inside:
            total = total + from_inner[s, zrows(z % 2), piece(h)].astype(f32)
        if s:
            result_out[s, :, piece(h)] = total.astype(bf16)
            result_copy(s, h).start()
        else:
            results[0:cp, piece(h)] = total.astype(bf16)

    def carry_copy(s):
        return remote(carries.at[0], carries.at[s], carry_send.at[s - 1], carry_recv.at[s - 1], ep_peer[s])

    def recurrence(services):
        state[...] = jnp.zeros_like(state)
        base[...] = jnp.zeros_like(base)
        n = CHUNK
        at = lax.broadcasted_iota(jnp.int32, (n, n), 0)
        of = lax.broadcasted_iota(jnp.int32, (n, n), 1)
        same = (at >= of) & (at // BLOCK_POSITIONS == of // BLOCK_POSITIONS)
        lower = jnp.where(same, 1.0, 0.0).astype(bf16)
        er = lax.broadcasted_iota(jnp.int32, (8, n), 0)
        pick_row = lax.broadcasted_iota(jnp.int32, (8, keys), 0)
        pick_head = lax.broadcasted_iota(jnp.int32, (8, keys), 1) // KEY_DIM
        pick = jnp.where((pick_row % heads == pick_head) & (pick_row < 3 * heads), 1.0, 0.0).astype(bf16)
        small = (BLOCK_POSITIONS, BLOCK_POSITIONS)
        causal = lax.broadcasted_iota(jnp.int32, small, 0) >= lax.broadcasted_iota(jnp.int32, small, 1)
        lane_head = lax.broadcasted_iota(jnp.int32, (BLOCK_POSITIONS, vals), 1) // VAL_DIM

        def chunk(i, _):
            for when, work in services.items():

                @pl.when(i == when)
                def _():
                    work()

            start = pl.multiple_of(i * n, n)
            here = pl.ds(start, n)
            qc = q[here, :].astype(f32)
            qc = qc / (1.0 + jnp.exp(-qc))
            key = gap_ref[...] / (1.0 + jnp.exp(f[here, :].astype(f32)))
            terms = jnp.zeros((8, n), f32)
            for h in range(heads):
                value = jnp.broadcast_to(extra_ref[h : h + 1, here], (8, n))
                one = value.astype(bf16).astype(f32)
                second = (value - one).astype(bf16).astype(f32)
                third = value - one - second
                terms = jnp.where(er == h, one, terms)
                terms = jnp.where(er == heads + h, second, terms)
                terms = jnp.where(er == 2 * heads + h, third, terms)
            extra = lax.dot_general(terms.astype(bf16), pick, TN, preferred_element_type=f32)
            log_forget = jnp.log(1.0 - key) + extra
            high = log_forget.astype(bf16)
            low = (log_forget - high.astype(f32)).astype(bf16)
            cumulative = jnp.dot(lower, high, preferred_element_type=f32) + jnp.dot(
                lower, low, preferred_element_type=f32
            )
            held = [state[h] for h in range(heads)]
            before = base[...]
            mid_at = BLOCK_POSITIONS // 2
            for b in range(n // BLOCK_POSITIONS):
                part = slice(b * BLOCK_POSITIONS, (b + 1) * BLOCK_POSITIONS)
                block = pl.ds(start + b * BLOCK_POSITIONS, BLOCK_POSITIONS)
                cum = cumulative[part]
                mid, last = cum[mid_at - 1 : mid_at], cum[BLOCK_POSITIONS - 1 :]
                q_part = qc[part]
                q_mid = (q_part * jnp.exp(cum - mid)).astype(bf16)
                k_mid = (key[part] * jnp.exp(mid - cum)).astype(bf16)
                qdec[block, :] = (q_part * jnp.exp(cum + before)).astype(bf16)
                decay_mid, decay_last, decay_rest = jnp.exp(mid), jnp.exp(last), jnp.exp(last - mid)
                before = before + last
                values = v[block, :]
                out = jnp.zeros((BLOCK_POSITIONS, vals), f32)
                for h in range(heads):
                    lanes = slice(h * KEY_DIM, (h + 1) * KEY_DIM)
                    across = lax.dot_general(
                        q_mid[:, lanes],
                        (held[h] * decay_mid[:, lanes]).astype(bf16),
                        NT,
                        preferred_element_type=f32,
                    )
                    scores = lax.dot_general(q_mid[:, lanes], k_mid[:, lanes], NT, preferred_element_type=f32)
                    scores = jnp.where(causal, scores, 0.0).astype(bf16)
                    within = jnp.dot(scores, values, preferred_element_type=f32)
                    out = jnp.where(lane_head == h, within + across, out)
                    update = lax.dot_general(values, k_mid[:, lanes], TN, preferred_element_type=f32)
                    held[h] = held[h] * decay_last[:, lanes] + update * decay_rest[:, lanes]
                rec[block, :] = out
            for h in range(heads):
                state[h] = held[h]
            base[...] = before
            return 0

        lax.fori_loop(0, length // n, chunk, 0)
        own = [state[h, h * VAL_DIM : (h + 1) * VAL_DIM, :] for h in range(heads)]
        carries[0, :VAL_DIM, :] = jnp.concatenate(own, axis=1).astype(bf16)
        total = jnp.exp(base[...])
        carries[0, VAL_DIM:, :] = jnp.broadcast_to(total, (16, keys)).astype(bf16)
        for s in range(1, places):
            carry_copy(s).start()

    chunk_rows = length // ROW_CHUNKS

    def rows_of(r):
        return pl.ds(r * chunk_rows, chunk_rows)

    def own_copy(r, side):
        here = mixed_all.at[z, side, rows_of(r)]
        return remote(here, here, own_send.at[r], own_recv.at[r], partner)

    def hop_right(src, r):
        here = mixed_all.at[src, c, rows_of(r)]
        to = {"tp": jnp.minimum(z + 1, last_z) * 2 + c}
        return remote(here, here, right_send.at[src, r], ag_recv.at[src, r], to)

    def hop_left(src, r):
        here = mixed_all.at[src, c, rows_of(r)]
        to = {"tp": jnp.maximum(z - 1, 0) * 2 + c}
        return remote(here, here, left_send.at[src, r], ag_recv.at[src, r], to)

    def ag_forward(src, r, side):
        here = mixed_all.at[src, side, rows_of(r)]
        return remote(here, here, agf_send.at[src, r], agf_recv.at[src, r], partner)

    def source(j, inside):
        at = (None, 2, 0, 3)[j] if inside else j
        return jnp.where(z < 2, at, last_z - at)

    def start_own(r):
        @pl.when(z < last_z)
        def _():
            hop_right(z, r).start()

        @pl.when(z > 0)
        def _():
            hop_left(z, r).start()

    def ag_step(j, inside, r):
        src = source(j, inside)
        hop_right(src, r).wait_recv()
        if inside:

            @pl.when(src < z)
            def _():
                hop_right(src, r).start()

            @pl.when(src > z)
            def _():
                hop_left(src, r).start()

        ag_forward(src, r, c).start()

    def gated():
        for s in range(1, places):
            carry_copy(s).wait_recv()
        total = jnp.zeros((VAL_DIM, keys), f32)
        for i in range(places):
            decay = carries[ep ^ i, VAL_DIM:, :].astype(f32)[:1]
            joined = total * decay + carries[ep ^ i, :VAL_DIM, :].astype(f32)
            total = jnp.where(i < ep, joined, total)
        lane_head = lax.broadcasted_iota(jnp.int32, total.shape, 1) // KEY_DIM
        for h in range(heads):
            held_state[h * VAL_DIM : (h + 1) * VAL_DIM, :] = jnp.where(lane_head == h, total, 0.0).astype(bf16)
        at = lax.broadcasted_iota(jnp.int32, (vals, vals), 0) // VAL_DIM
        of = lax.broadcasted_iota(jnp.int32, (vals, vals), 1) // VAL_DIM
        average = jnp.where(at == of, 1.0 / VAL_DIM, 0.0).astype(bf16)
        for r in range(ROW_CHUNKS):
            here = rows_of(r)
            whole = rec[here, :] + lax.dot_general(
                qdec[here, :], held_state[...], NT, preferred_element_type=f32
            )
            square = whole * whole
            high = square.astype(bf16)
            low = (square - high.astype(f32)).astype(bf16)
            mean = jnp.dot(high, average, preferred_element_type=f32) + jnp.dot(
                low, average, preferred_element_type=f32
            )
            opened = gate[here, :].astype(f32)
            opened = opened / (1.0 + jnp.exp(-opened))
            mixed = (whole * lax.rsqrt(mean + epsilon) * head_gain_ref[...] * opened).astype(bf16)
            mixed_all[z, c, here, :] = mixed

            @pl.when(is_inner)
            def _():
                start_own(r)

            own_copy(r, c).start()

    def out_copy(r):
        return pltpu.make_async_copy(out_buf.at[rows_of(r)], out_ref.at[rows_of(r)], out_sem.at[r])

    def moe_copy():
        return pltpu.make_async_copy(moe_buf, moe_ref, out_sem.at[ROW_CHUNKS])

    def project(j, inside, r):
        src = source(j, inside) if j else z
        if j:
            ag_forward(src, r, oc).wait_recv()
        else:
            own_copy(r, oc).wait_recv()
        here = rows_of(r)
        weight = wo[pl.ds(pl.multiple_of(src * 2 * vc, LANES), 2 * vc), :]
        both = jnp.concatenate([mixed_all[src, 0, here, :], mixed_all[src, 1, here, :]], axis=1)
        part = jnp.dot(both, weight, preferred_element_type=f32)
        if j:
            part = part + out_acc[here, :]
        if j == last_z:
            out_buf[here, :] = part.astype(bf16)
            out_copy(r).start()
        else:
            out_acc[here, :] = part

    def swap_copy():
        return remote(
            combined.at[pl.ds(pl.multiple_of(oc * sub, 16), sub)],
            moe_buf.at[:, half(c)], swap_send.at[0], swap_recv.at[0], partner,
        )

    def swap_in():
        return remote(
            combined.at[pl.ds(pl.multiple_of(oc * sub, 16), sub)],
            moe_buf.at[:, half(oc)], swap_send.at[0], swap_recv.at[0], partner,
        )

    def combine():
        lanes = pl.ds(pl.multiple_of(z * two, LANES), two)
        where_to, first, second = targets(lanes)
        weight = jnp.where(first, jnp.broadcast_to(weight_ref[0:1, lanes], (8, two)), 0.0) + jnp.where(
            second, jnp.broadcast_to(weight_ref[1:2, lanes], (8, two)), 0.0
        )
        high = weight.astype(bf16).astype(f32)
        low = weight - high
        picks = [slot_row == where_to[s : s + 1, :] for s in range(places)]
        coarse = jnp.concatenate(
            [jnp.where(picks[s], high[s : s + 1, :], 0.0).astype(bf16) for s in range(places)], axis=0
        )
        fine = jnp.concatenate(
            [jnp.where(picks[s], low[s : s + 1, :], 0.0).astype(bf16) for s in range(places)], axis=0
        )
        for s in range(1, places):
            for h in range(pieces):
                result_copy(s, h).wait_recv()
        total = lax.dot_general(coarse, results[...], TN, preferred_element_type=f32) + lax.dot_general(
            fine, results[...], TN, preferred_element_type=f32
        )
        combined[...] = total.astype(bf16)
        swap_copy().start()

    def finish():
        moe_buf[:, half(c)] = combined[pl.ds(pl.multiple_of(c * sub, 16), sub), :]
        swap_in().wait_recv()
        moe_copy().start()

    chunks = range(ROW_CHUNKS)
    both = range(pieces)
    for j in range(blocks_f):
        loads[("wg", j)].wait()
        loads[("wu", j)].wait()
    moe(0)
    for name in ("q", "f", "v", "gap", "extra"):
        loads[name].wait()

    def take(s, at):
        for g in at:
            forward(s, g)

    def second(s):
        for h in both:
            stage2(s, h)

    def third(s):
        for h in both:
            stage3(s, h)

    def mates(s):
        @pl.when(is_end)
        def _():
            for h in both:
                mate_copy(s, h).start()

    def starts(at):
        @pl.when(is_end)
        def _():
            for r in at:
                start_own(r)

    recurrence(
        {
            1: lambda: (stage1(0), mates(0)),
            3: lambda: (take(1, [0]), take(2, [0])),
            5: lambda: (take(1, [1]), take(2, [1])),
            6: inner(lambda: stage2(0, 0)),
            7: lambda: (take(1, [2]), take(2, [2])),
        }
    )
    take(1, [3])
    take(2, [3])
    inner(lambda: stage2(0, 1))()
    moe(1)
    loads["gate"].wait()
    loads["head_gain"].wait()
    gated()
    stage1(1)
    moe(2)
    inner(lambda: third(0))()
    stage1(2)
    take(3, range(pairs))
    moe(3)
    loads["wo"].wait()
    loads["weight"].wait()
    stage1(3)

    @pl.when(is_end)
    def _():
        for r in chunks:
            start_own(r)
        for s in range(1, places):
            for h in both:
                mate_copy(s, h).start()
        for r in chunks:
            project(0, False, r)
            ag_step(1, False, r)
        for h in both:
            stage4(0, h, False)
        for r in chunks:
            ag_step(2, False, r)
            project(1, False, r)
        for s in (1, 2):
            for h in both:
                stage4(s, h, False)
        for r in chunks:
            project(2, False, r)
        for r in (0, 1):
            ag_step(3, False, r)
        for h in both:
            stage4(3, h, False)
        for r in (2, 3):
            ag_step(3, False, r)
        for r in chunks:
            project(3, False, r)

    @pl.when(is_inner)
    def _():
        second(1)
        for r in chunks:
            project(0, True, r)
            ag_step(1, True, r)
        stage2(2, 0)
        stage3(1, 0)
        stage2(2, 1)
        stage3(1, 1)
        for r in chunks:
            project(1, True, r)
        stage2(3, 0)
        stage3(2, 0)
        stage2(3, 1)
        ag_step(2, True, 0)
        stage3(2, 1)
        ag_step(2, True, 1)
        ag_step(3, True, 0)
        stage3(3, 0)
        ag_step(2, True, 2)
        ag_step(3, True, 1)
        stage3(3, 1)
        ag_step(2, True, 3)
        ag_step(3, True, 2)
        ag_step(3, True, 3)
        for r in chunks:
            project(2, True, r)
        for s in range(places):
            for h in both:
                stage4(s, h, True)
        for r in chunks:
            project(3, True, r)

    combine()
    finish()

    for s in range(1, places):
        for g in range(pairs):
            dispatch(s, g).wait_send()
            dispatch_forward(s, g, c).wait_send()
        carry_copy(s).wait_send()
        for h in both:
            result_copy(s, h).wait_send()
    for s in range(places):
        for h in both:
            pair_copy(s, h).wait_send()
            mate_copy(s, h).wait_send()

            @pl.when(is_end)
            def _():
                end_copy(s, h).wait_send()

            @pl.when(is_inner)
            def _():
                inner_copy(s, h).wait_send()

    for r in chunks:
        own_copy(r, c).wait_send()
        out_copy(r).wait()
        for src in range(pairs):

            @pl.when((src <= z) & (z < last_z))
            def _():
                hop_right(src, r).wait_send()

            @pl.when((src >= z) & (z > 0))
            def _():
                hop_left(src, r).wait_send()

            @pl.when(src != z)
            def _():
                ag_forward(src, r, c).wait_send()

    swap_copy().wait_send()
    moe_copy().wait()


def on_device(*arrays):
    (
        query, forget, values, gate, gap, extra, head_gain, out_weight,
        tokens, norm_gain, index, weight, gate_weight, up_weight, down_weight,
    ) = arrays
    places, groups = lax.axis_size("ep"), lax.axis_size("tp")
    pairs = groups // 2
    length, keys = query.shape
    vals = values.shape[1]
    count, width = tokens.shape
    hidden = gate_weight.shape[2]
    sub = count // groups
    experts_all = gate_weight.shape[0] * places
    capacity = max(2, sub * TOPK * 5 // (4 * experts_all))
    fits = (
        places == 4
        and groups == 8
        and gate_weight.shape[0] == 1
        and 2 * sub == LANES
        and capacity % 8 == 0
        and capacity <= sub
        and vals == LANES
        and keys == 2 * KEY_DIM
        and length % (ROW_CHUNKS * CHUNK) == 0
        and hidden % LANES == 0
        and width % 512 == 0
    )
    if not fits:
        return general(*arrays)
    heads = keys // KEY_DIM
    cp = 2 * capacity
    rows_all = pairs * cp
    hw = width // 2
    features = out_weight.shape[1]
    bf16, f32 = jnp.bfloat16, jnp.float32
    vmem = pl.BlockSpec(memory_space=pltpu.VMEM)
    anywhere = pl.BlockSpec(memory_space=pl.ANY)
    dma = pltpu.SemaphoreType.DMA
    small = [index.T, weight.T, norm_gain.reshape(1, width), gap.reshape(1, keys), extra.T, head_gain.reshape(1, vals)]
    scratch = [pltpu.VMEM(a.shape, a.dtype) for a in small]
    scratch += [
        pltpu.VMEM((count, width), bf16),
        pltpu.VMEM((length, keys), bf16),
        pltpu.VMEM((length, keys), bf16),
        pltpu.VMEM((length, vals), bf16),
        pltpu.VMEM((length, vals), bf16),
        pltpu.VMEM(out_weight.shape, bf16),
        pltpu.VMEM((hidden // LANES, width, 2 * LANES), bf16),
        pltpu.VMEM((hidden, width), bf16),
        pltpu.VMEM((places - 1, rows_all, hw), bf16),
        pltpu.VMEM((places, rows_all, width), bf16),
        pltpu.VMEM((rows_all, hidden), bf16),
        pltpu.VMEM((places, rows_all, hw), bf16),
        pltpu.VMEM((places, rows_all, hw), bf16),
        pltpu.VMEM((places, rows_all, hw), bf16),
        pltpu.VMEM((places, 2 * cp, hw), bf16),
        pltpu.VMEM((places, cp, hw), bf16),
        pltpu.VMEM((places, 2 * cp, hw), bf16),
        pltpu.VMEM((places, cp, hw), bf16),
        pltpu.VMEM((places * cp, hw), bf16),
        pltpu.VMEM((2 * sub, hw), bf16),
        pltpu.VMEM((sub, width), bf16),
        pltpu.VMEM((heads, vals, KEY_DIM), f32),
        pltpu.VMEM((1, keys), f32),
        pltpu.VMEM((places, VAL_DIM + 16, keys), bf16),
        pltpu.VMEM((length, vals), f32),
        pltpu.VMEM((length, keys), bf16),
        pltpu.VMEM((vals, keys), bf16),
        pltpu.VMEM((pairs, 2, length, vals), bf16),
        pltpu.VMEM((length, features), f32),
        pltpu.VMEM((length, features), bf16),
    ]
    n_loads = pairs + 2 * (hidden // LANES) + 12
    peers = places - 1
    sems = [dma((n_loads,))]
    sems += [dma((peers, pairs))] * 4 + [dma((places, 2))] * 8 + [dma((peers, 2))] * 2 + [dma((1,))] * 2
    sems += [dma((peers,))] * 2 + [dma((ROW_CHUNKS,))] * 2 + [dma((pairs, ROW_CHUNKS))] * 5 + [dma((ROW_CHUNKS + 1,))]
    outputs = pl.pallas_call(
        fused_kernel,
        in_specs=[anywhere] * 15,
        out_specs=[anywhere, anywhere],
        out_shape=[
            jax.ShapeDtypeStruct((length, features), bf16),
            jax.ShapeDtypeStruct((sub, width), bf16),
        ],
        scratch_shapes=scratch + sems,
        compiler_params=pltpu.CompilerParams(
            collective_id=0, has_side_effects=True, vmem_limit_bytes=64 * 1024 * 1024 - 65536
        ),
        name="fused_layer",
    )(
        *small, tokens, query, forget, values, gate, out_weight,
        gate_weight, up_weight, down_weight,
    )
    parts = [(0, r * length // 4, length // 4) for r in range(4)] + [(1, 0, sub)]

    def deliver(first, second, out_first, out_second, buf, small_buf, sem_in, sem_out):
        sources, targets, bufs = (first, second), (out_first, out_second), (buf, small_buf)
        into = [
            pltpu.make_async_copy(sources[w].at[pl.ds(a, n)], bufs[w].at[pl.ds(a, n)], sem_in.at[i])
            for i, (w, a, n) in enumerate(parts)
        ]
        outof = [
            pltpu.make_async_copy(bufs[w].at[pl.ds(a, n)], targets[w].at[pl.ds(a, n)], sem_out.at[i])
            for i, (w, a, n) in enumerate(parts)
        ]
        for copy in into:
            copy.start()
        for i, copy in enumerate(into):
            copy.wait()
            outof[i].start()
        for copy in outof:
            copy.wait()

    return tuple(
        pl.pallas_call(
            deliver,
            in_specs=[anywhere] * 2,
            out_specs=[anywhere] * 2,
            out_shape=[jax.ShapeDtypeStruct((length, features), bf16), jax.ShapeDtypeStruct((sub, width), bf16)],
            scratch_shapes=[
                pltpu.VMEM((length, features), bf16),
                pltpu.VMEM((sub, width), bf16),
                dma((len(parts),)),
                dma((len(parts),)),
            ],
            name="deliver",
        )(*outputs)
    )


def solution(mesh):
    placed = (
        P("ep", "tp"),
        P("ep", "tp"),
        P("ep", "tp"),
        P("ep", "tp"),
        P("tp"),
        P("ep", "tp"),
        P("tp"),
        P(None, "tp"),
        P("ep", None),
        P(),
        P("ep", None),
        P("ep", None),
        P("ep", None, "tp"),
        P("ep", None, "tp"),
        P("ep", "tp", None),
    )
    return jax.shard_map(
        on_device,
        mesh=mesh,
        in_specs=placed,
        out_specs=(P("ep", "tp"), P(("ep", "tp"), None)),
        check_vma=False,
    )
```

```python
import functools

import jax
import jax.numpy as jnp
from jax import lax
from jax.experimental import pallas as pl
from jax.experimental.pallas import tpu as pltpu
from jax.sharding import PartitionSpec as P

KEY_DIM = 128
VAL_DIM = 64
BLOCK_POSITIONS = 64
TOPK = 2


epsilon = 1e-06


CHUNK = 256
NT = (((1,), (1,)), ((), ()))
TN = (((0,), (0,)), ((), ()))


def local_kernel(heads, q_ref, f_ref, v_ref, gap_ref, extra_ref, rec_ref, qdec_ref, carry_ref, state, base):
    step = pl.program_id(0)

    @pl.when(step == 0)
    def _():
        state[...] = jnp.zeros_like(state)
        base[...] = jnp.zeros_like(base)

    rows, vals = v_ref.shape
    q = q_ref[...].astype(jnp.float32)
    q = q / (1.0 + jnp.exp(-q))
    key = gap_ref[...] / (1.0 + jnp.exp(f_ref[...].astype(jnp.float32)))
    extra = extra_ref[...]
    log_forget = jnp.log(1.0 - key) + jnp.concatenate(
        [jnp.broadcast_to(extra[:, h : h + 1], (rows, KEY_DIM)) for h in range(heads)], axis=1
    )
    at = lax.broadcasted_iota(jnp.int32, (rows, rows), 0)
    of = lax.broadcasted_iota(jnp.int32, (rows, rows), 1)
    lower = jnp.where((at >= of) & (at // BLOCK_POSITIONS == of // BLOCK_POSITIONS), 1.0, 0.0)
    lower = lower.astype(jnp.bfloat16)
    high = log_forget.astype(jnp.bfloat16)
    low = (log_forget - high.astype(jnp.float32)).astype(jnp.bfloat16)
    cumulative = jnp.dot(lower, high, preferred_element_type=jnp.float32) + jnp.dot(
        lower, low, preferred_element_type=jnp.float32
    )
    causal = lax.broadcasted_iota(
        jnp.int32, (BLOCK_POSITIONS, BLOCK_POSITIONS), 0
    ) >= lax.broadcasted_iota(jnp.int32, (BLOCK_POSITIONS, BLOCK_POSITIONS), 1)
    lane_head = lax.broadcasted_iota(jnp.int32, (BLOCK_POSITIONS, vals), 1) // VAL_DIM
    held = [state[h] for h in range(heads)]
    before = base[...]
    half = BLOCK_POSITIONS // 2
    for b in range(rows // BLOCK_POSITIONS):
        part = slice(b * BLOCK_POSITIONS, (b + 1) * BLOCK_POSITIONS)
        cum = cumulative[part]
        mid, last = cum[half - 1 : half], cum[BLOCK_POSITIONS - 1 :]
        q_part = q[part]
        q_mid = (q_part * jnp.exp(cum - mid)).astype(jnp.bfloat16)
        k_mid = (key[part] * jnp.exp(mid - cum)).astype(jnp.bfloat16)
        qdec_ref[part, :] = (q_part * jnp.exp(cum + before)).astype(jnp.bfloat16)
        decay_mid, decay_last, decay_rest = jnp.exp(mid), jnp.exp(last), jnp.exp(last - mid)
        before = before + last
        values = v_ref[part, :]
        out = jnp.zeros((BLOCK_POSITIONS, vals), jnp.float32)
        for h in range(heads):
            lanes = slice(h * KEY_DIM, (h + 1) * KEY_DIM)
            across = lax.dot_general(
                q_mid[:, lanes],
                (held[h] * decay_mid[:, lanes]).astype(jnp.bfloat16),
                NT,
                preferred_element_type=jnp.float32,
            )
            scores = lax.dot_general(
                q_mid[:, lanes], k_mid[:, lanes], NT, preferred_element_type=jnp.float32
            )
            scores = jnp.where(causal, scores, 0.0).astype(jnp.bfloat16)
            within = jnp.dot(scores, values, preferred_element_type=jnp.float32)
            out = jnp.where(lane_head == h, within + across, out)
            update = lax.dot_general(
                values, k_mid[:, lanes], TN, preferred_element_type=jnp.float32
            )
            held[h] = held[h] * decay_last[:, lanes] + update * decay_rest[:, lanes]
        rec_ref[part, :] = out
    for h in range(heads):
        state[h] = held[h]
    base[...] = before

    @pl.when(step == pl.num_programs(0) - 1)
    def _():
        own = [held[h][h * VAL_DIM : (h + 1) * VAL_DIM] for h in range(heads)]
        carry_ref[:VAL_DIM, :] = jnp.concatenate(own, axis=1).astype(jnp.bfloat16)
        total = jnp.exp(before)
        carry_ref[VAL_DIM:, :] = jnp.broadcast_to(total, (16, total.shape[1])).astype(jnp.bfloat16)


def local_recurrence(query, forget, values, gap, extra):
    length, keys = query.shape
    heads, vals = keys // KEY_DIM, values.shape[1]

    def chunk(width):
        return pl.BlockSpec((CHUNK, width), lambda i: (i, 0))

    return pl.pallas_call(
        functools.partial(local_kernel, heads),
        grid=(length // CHUNK,),
        in_specs=[
            chunk(keys),
            chunk(keys),
            chunk(vals),
            pl.BlockSpec((1, keys), lambda i: (0, 0)),
            chunk(heads),
        ],
        out_specs=[
            chunk(vals),
            chunk(keys),
            pl.BlockSpec((VAL_DIM + 16, keys), lambda i: (0, 0)),
        ],
        out_shape=[
            jax.ShapeDtypeStruct((length, vals), jnp.float32),
            jax.ShapeDtypeStruct((length, keys), jnp.bfloat16),
            jax.ShapeDtypeStruct((VAL_DIM + 16, keys), jnp.bfloat16),
        ],
        scratch_shapes=[
            pltpu.VMEM((heads, vals, KEY_DIM), jnp.float32),
            pltpu.VMEM((1, keys), jnp.float32),
        ],
        cost_estimate=pl.CostEstimate(
            flops=10_000_000_000, bytes_accessed=6_000_000, transcendentals=3_000_000
        ),
        name="local_recurrence",
    )(query, forget, values, gap.reshape(1, keys), extra)


def gate_kernel(heads, places, place_ref, rec_ref, qdec_ref, carry_ref, gain_ref, gate_ref, out_ref, held):
    rows, vals = rec_ref.shape

    @pl.when(pl.program_id(0) == 0)
    def _():
        place = place_ref[0]
        total = jnp.zeros((VAL_DIM, heads * KEY_DIM), jnp.float32)
        for i in range(places):
            decay = carry_ref[i, VAL_DIM:, :].astype(jnp.float32)[:1]
            joined = total * decay + carry_ref[i, :VAL_DIM, :].astype(jnp.float32)
            total = jnp.where(i < place, joined, total)
        lane_head = lax.broadcasted_iota(jnp.int32, total.shape, 1) // KEY_DIM
        for h in range(heads):
            held[h * VAL_DIM : (h + 1) * VAL_DIM, :] = jnp.where(lane_head == h, total, 0.0).astype(
                jnp.bfloat16
            )

    rec = rec_ref[...] + lax.dot_general(
        qdec_ref[...], held[...], NT, preferred_element_type=jnp.float32
    )
    at = lax.broadcasted_iota(jnp.int32, (vals, vals), 0) // VAL_DIM
    of = lax.broadcasted_iota(jnp.int32, (vals, vals), 1) // VAL_DIM
    average = jnp.where(at == of, 1.0 / VAL_DIM, 0.0).astype(jnp.bfloat16)
    square = rec * rec
    high = square.astype(jnp.bfloat16)
    low = (square - high.astype(jnp.float32)).astype(jnp.bfloat16)
    mean = jnp.dot(high, average, preferred_element_type=jnp.float32) + jnp.dot(
        low, average, preferred_element_type=jnp.float32
    )
    gate = gate_ref[...].astype(jnp.float32)
    gate = gate / (1.0 + jnp.exp(-gate))
    out_ref[...] = (rec * lax.rsqrt(mean + epsilon) * gain_ref[...] * gate).astype(jnp.bfloat16)


def gated_output(rec, qdec, carries, gain, gate):
    length, vals = rec.shape
    keys = qdec.shape[1]
    heads = keys // KEY_DIM
    rows = 2 * CHUNK

    def chunk(width):
        return pl.BlockSpec((rows, width), lambda i: (i, 0))

    return pl.pallas_call(
        functools.partial(gate_kernel, heads, carries.shape[0]),
        grid=(length // rows,),
        in_specs=[
            pl.BlockSpec(memory_space=pltpu.SMEM),
            chunk(vals),
            chunk(keys),
            pl.BlockSpec(carries.shape, lambda i: (0, 0, 0)),
            pl.BlockSpec((1, vals), lambda i: (0, 0)),
            chunk(vals),
        ],
        out_specs=chunk(vals),
        out_shape=jax.ShapeDtypeStruct((length, vals), jnp.bfloat16),
        scratch_shapes=[pltpu.VMEM((vals, keys), jnp.bfloat16)],
        cost_estimate=pl.CostEstimate(
            flops=2_000_000_000, bytes_accessed=3_000_000, transcendentals=1_000_000
        ),
        name="gated_output",
    )(lax.axis_index("ep").reshape(1), rec, qdec, carries, gain.reshape(1, vals), gate)


def norm_rows(tokens, row_gain):
    tokens_float = tokens.astype(jnp.float32)
    factor = lax.rsqrt(jnp.mean(tokens_float * tokens_float, axis=-1, keepdims=True) + epsilon)
    return (tokens_float * factor * row_gain).astype(jnp.bfloat16)


def slot_positions(blocks, experts_all):
    flattened = blocks.reshape(blocks.shape[0], -1)
    onehot = (flattened[..., None] == jnp.arange(experts_all, dtype=jnp.int32)).astype(jnp.int32)
    earlier = jnp.cumsum(onehot, axis=1) - onehot
    return jnp.sum(earlier * onehot, axis=-1).reshape(blocks.shape)


def fill_slots(rows_in, blocks, slot_ids, experts_all, capacity):
    groups = blocks.shape[0]
    sub_rows = blocks.shape[1]
    group_ids = jnp.arange(groups, dtype=jnp.int32)[:, None, None]
    target = (group_ids * experts_all + blocks) * capacity + slot_ids
    sources = jnp.broadcast_to(
        jnp.arange(sub_rows, dtype=jnp.int32)[None, :, None] + group_ids * sub_rows, blocks.shape
    )
    lookup = (
        jnp.full((groups * experts_all * capacity,), -1, jnp.int32)
        .at[target.reshape(-1)]
        .set(sources.reshape(-1))
    )
    gathered = rows_in.reshape(groups * sub_rows, -1)[jnp.maximum(lookup, 0)]
    filled = jnp.where((lookup >= 0)[:, None], gathered, jnp.zeros((), gathered.dtype))
    return filled.reshape(groups, experts_all, capacity, -1)


def general(
    query_preactivation,
    forget_preactivation,
    value_input_rows,
    output_gate_preactivation,
    forget_floor_gap,
    extra_log_forget,
    head_output_gain,
    mixer_output_weight,
    second_batch_tokens,
    feedforward_norm_gain,
    chosen_expert_index,
    chosen_expert_weight,
    expert_gate_weight,
    expert_up_weight,
    expert_down_weight,
):
    local_experts = expert_gate_weight.shape[0]
    places = lax.axis_size("ep")
    experts_all = local_experts * places
    groups = lax.axis_size("tp")
    width = second_batch_tokens.shape[1]
    sub_rows = second_batch_tokens.shape[0] // groups
    capacity = max(2, sub_rows * TOPK * 5 // (4 * experts_all))
    place = lax.axis_index("ep")
    position = lax.axis_index("tp")
    pairs = groups // 2
    side = lax.rem(position, 2)

    all_routes = chosen_expert_index.reshape(pairs, 2, sub_rows, TOPK)
    routes = lax.dynamic_index_in_dim(all_routes, side, 1, False)
    all_tokens = second_batch_tokens.reshape(pairs, 2, sub_rows, width)
    tokens = lax.dynamic_index_in_dim(all_tokens, side, 1, False)
    slots = slot_positions(routes, experts_all)
    outgoing = fill_slots(
        norm_rows(tokens, feedforward_norm_gain), routes, slots, experts_all, capacity
    )
    outgoing, query_preactivation = lax.optimization_barrier((outgoing, query_preactivation))
    outgoing = outgoing.reshape(pairs, places, local_experts, capacity, width)
    arrived = []
    for step in range(places):
        block = lax.dynamic_index_in_dim(outgoing, place ^ step, 1, False)
        if step:
            block = lax.ppermute(block, "ep", [(i, i ^ step) for i in range(places)])
        arrived.append(block)
    partners = [(i, i ^ 1) for i in range(groups)]
    shape = (pairs, places, local_experts, capacity, width)
    others = [lax.ppermute(block, "tp", partners) for block in arrived]
    own_side = jnp.stack(arrived, axis=1)
    other_side = jnp.stack(others, axis=1)

    recurrent, query_decayed, carry = local_recurrence(
        query_preactivation,
        forget_preactivation,
        value_input_rows,
        forget_floor_gap,
        extra_log_forget,
    )
    carries = lax.all_gather(carry, "ep")
    mixed = gated_output(
        recurrent, query_decayed, carries, head_output_gain, output_gate_preactivation
    )
    mixed_all = lax.all_gather(mixed, "tp", axis=1, tiled=True)

    def experts(rows):
        gate_part = jnp.einsum(
            "tsecd,edf->tsecf", rows, expert_gate_weight, preferred_element_type=jnp.float32
        )
        up_part = jnp.einsum(
            "tsecd,edf->tsecf", rows, expert_up_weight, preferred_element_type=jnp.float32
        )
        hidden = (jax.nn.silu(gate_part) * up_part).astype(jnp.bfloat16)
        product = jnp.einsum(
            "tsecf,efd->tsecd", hidden, expert_down_weight, preferred_element_type=jnp.float32
        )
        return product.astype(jnp.bfloat16)

    other_side, mixed = lax.optimization_barrier((other_side, mixed))
    for_partner = experts(other_side)
    own_side, for_partner = lax.optimization_barrier((own_side, for_partner))
    from_partner = lax.ppermute(for_partner, "tp", partners)
    product = experts(own_side).astype(jnp.float32) + from_partner.astype(jnp.float32)
    product, mixed_all = lax.optimization_barrier((product.astype(jnp.bfloat16), mixed_all))
    to_return = lax.psum_scatter(
        product,
        "tp",
        scatter_dimension=0,
        tiled=True,
        axis_index_groups=[list(range(c, groups, 2)) for c in range(2)],
    )
    to_return = to_return.reshape(shape[1:])
    mixer_output_first = jnp.dot(
        mixed_all, mixer_output_weight, preferred_element_type=jnp.float32
    ).astype(jnp.bfloat16)
    returned = []
    for step in range(places):
        block = to_return[step]
        if step:
            block = lax.ppermute(block, "ep", [(i, i ^ step) for i in range(places)])
        returned.append(block)
    results = jnp.concatenate(returned, axis=0).reshape(experts_all * capacity, width)
    own_routes = lax.dynamic_index_in_dim(routes, position // 2, 0, False)
    own_slots = lax.dynamic_index_in_dim(slots, position // 2, 0, False)
    own_weights = lax.dynamic_slice_in_dim(chosen_expert_weight, position * sub_rows, sub_rows, 0)
    holder = (own_routes // local_experts) ^ place
    flat_index = (holder * local_experts + own_routes % local_experts) * capacity + own_slots
    combined = jnp.zeros((sub_rows, width), jnp.float32)
    for ranked in range(TOPK):
        combined = (
            combined
            + results[flat_index[:, ranked]].astype(jnp.float32)
            * own_weights[:, ranked : ranked + 1]
        )
    return (mixer_output_first, combined.astype(jnp.bfloat16))


MESH = pl.DeviceIdType.MESH
LANES = 128
ROW_CHUNKS = 4


def fused_kernel(
    idx_hbm, weight_hbm, norm_gain_hbm, gap_hbm, extra_hbm, head_gain_hbm,
    tok_hbm, q_hbm, f_hbm, v_hbm, g_hbm, wo_hbm, wg_hbm, wu_hbm, wd_hbm,
    out_ref, moe_ref,
    idx_ref, weight_ref, norm_gain_ref, gap_ref, extra_ref, head_gain_ref,
    tok, q, f, v, gate, wo, wgu, wd,
    send_rows, rows, hidden, pair_out, pair_in, psum, from_end, from_mate, from_inner,
    result_out, results, combined, moe_buf,
    state, base, carries, rec, qdec, held_state, mixed_all, out_acc, out_buf,
    load_sem, disp_send, disp_recv, dfwd_send, dfwd_recv, pair_send, pair_recv,
    end_send, end_recv, mate_send, mate_recv, inner_send, inner_recv,
    ret_send, ret_recv, swap_send, swap_recv, carry_send, carry_recv,
    own_send, own_recv, right_send, left_send, ag_recv, agf_send, agf_recv, out_sem,
):
    f32, bf16 = jnp.float32, jnp.bfloat16
    ep = lax.axis_index("ep")
    tp = lax.axis_index("tp")
    z, c = tp // 2, tp % 2
    last_z = mixed_all.shape[0] - 1
    oc = 1 - c
    mate = z + 1 - 2 * (z % 2)
    is_end = (z == 0) | (z == last_z)
    is_inner = (z > 0) & (z < last_z)
    places = rows.shape[0]
    steps = places
    pairs = mixed_all.shape[0]
    two = idx_ref.shape[1] // pairs
    sub = two // 2
    width = tok.shape[1]
    hw = width // 2
    rows_all = rows.shape[1]
    cp = rows_all // pairs
    cap = cp // 2
    length, keys = q.shape
    vals = v.shape[1]
    heads = keys // KEY_DIM
    blocks_f = wgu.shape[0]
    vc = vals
    ep_peer = [{"ep": ep ^ s} for s in range(places)]
    partner = {"tp": z * 2 + oc}
    mate_dev = {"tp": mate * 2 + c}
    across_dev = {"tp": (pairs - 1 - z) * 2 + c}

    pieces = 2
    pw = hw // pieces

    def piece(h):
        return pl.ds(h * pw, pw)

    def half(i):
        return pl.ds(pl.multiple_of(i * hw, LANES), hw)

    def vcols(i):
        return pl.ds(pl.multiple_of(i * vc, LANES), vc)

    def zrows(d, n=1):
        return pl.ds(pl.multiple_of(d * cp, 16), n * cp)

    def remote(src, dst, ssem, rsem, dev):
        return pltpu.make_async_remote_copy(
            src_ref=src, dst_ref=dst, send_sem=ssem, recv_sem=rsem, device_id=dev, device_id_type=MESH
        )

    barrier = pltpu.get_barrier_semaphore()
    for dev in ep_peer[1:] + [partner]:
        pl.semaphore_signal(barrier, inc=1, device_id=dev, device_id_type=MESH)

    @pl.when(z > 0)
    def _():
        pl.semaphore_signal(barrier, inc=1, device_id={"tp": tp - 2}, device_id_type=MESH)

    @pl.when(z < last_z)
    def _():
        pl.semaphore_signal(barrier, inc=1, device_id={"tp": tp + 2}, device_id_type=MESH)

    loads = {}

    def load(name, src, dst):
        copy = pltpu.make_async_copy(src, dst, load_sem.at[len(loads)])
        copy.start()
        loads[name] = copy

    load("idx", idx_hbm, idx_ref)
    load("norm_gain", norm_gain_hbm, norm_gain_ref)
    for g in range(pairs):
        part = pl.ds(g * two, two)
        load(("tok", g), tok_hbm.at[part], tok.at[part])
    for j in range(blocks_f):
        cols = pl.ds(j * LANES, LANES)
        load(("wg", j), wg_hbm.at[0, :, cols], wgu.at[j, :, pl.ds(0, LANES)])
        load(("wu", j), wu_hbm.at[0, :, cols], wgu.at[j, :, pl.ds(LANES, LANES)])
    load("wd", wd_hbm.at[0], wd)
    load("weight", weight_hbm, weight_ref)
    load("gap", gap_hbm, gap_ref)
    load("extra", extra_hbm, extra_ref)
    load("head_gain", head_gain_hbm, head_gain_ref)
    load("q", q_hbm, q)
    load("f", f_hbm, f)
    load("v", v_hbm, v)
    load("gate", g_hbm, gate)
    load("wo", wo_hbm, wo)

    tri_a = lax.broadcasted_iota(jnp.int32, (two, two), 0)
    tri_b = lax.broadcasted_iota(jnp.int32, (two, two), 1)
    earlier = jnp.where((tri_a < tri_b) & (tri_a // sub == tri_b // sub), 1.0, 0.0).astype(bf16)
    lane_side = lax.broadcasted_iota(jnp.int32, (8, two), 1) // sub
    slot_row = lax.broadcasted_iota(jnp.int32, (cp, two), 0).astype(f32)
    expert_row = ep ^ lax.broadcasted_iota(jnp.int32, (8, two), 0)

    def targets(lanes):
        first = jnp.broadcast_to(idx_ref[0:1, lanes], (8, two)) == expert_row
        second = jnp.broadcast_to(idx_ref[1:2, lanes], (8, two)) == expert_row
        match = first | second
        before = jnp.dot(jnp.where(match, 1.0, 0.0).astype(bf16), earlier, preferred_element_type=f32)
        where_to = jnp.where(match, before + (lane_side * cap).astype(f32), -1.0)
        return where_to, first, second

    def dispatch(s, g):
        return remote(
            send_rows.at[s - 1, zrows(g)], rows.at[s, zrows(g), half(c)],
            disp_send.at[s - 1, g], disp_recv.at[s - 1, g], ep_peer[s],
        )

    def dispatch_forward(s, g, side):
        here = rows.at[s, zrows(g), half(side)]
        return remote(here, here, dfwd_send.at[s - 1, g], dfwd_recv.at[s - 1, g], partner)

    loads["idx"].wait()
    loads["norm_gain"].wait()
    for g in range(pairs):
        part = slice(g * two, (g + 1) * two)
        loads[("tok", g)].wait()
        tokens = tok[part, :].astype(f32)
        factor = lax.rsqrt(jnp.mean(tokens * tokens, axis=-1, keepdims=True) + epsilon)
        tok[part, :] = (tokens * factor * norm_gain_ref[...]).astype(bf16)
        where_to, _, _ = targets(slice(g * two, (g + 1) * two))
        onehots = [
            jnp.where(slot_row == where_to[s : s + 1, :], 1.0, 0.0).astype(bf16) for s in range(places)
        ]
        own_half = tok[part, half(c)]
        for s in range(1, places):
            send_rows[s - 1, g * cp : (g + 1) * cp, :] = jnp.dot(
                onehots[s], own_half, preferred_element_type=f32
            ).astype(bf16)
        if g == 0:
            pl.semaphore_wait(barrier, jnp.where(is_end, places + 1, places + 2))
        for s in (1, 2):
            dispatch(s, g).start()
        rows[0, g * cp : (g + 1) * cp, :] = jnp.dot(
            onehots[0], tok[part, :], preferred_element_type=f32
        ).astype(bf16)
    for g in range(pairs):
        dispatch(3, g).start()

    def forward(s, g):
        dispatch(s, g).wait_recv()
        dispatch_forward(s, g, c).start()

    def pair_copy(s, h):
        return remote(
            pair_out.at[s, :, piece(h)], pair_in.at[s, :, piece(h)], pair_send.at[s, h], pair_recv.at[s, h], partner
        )

    def moe(s):
        if s:
            for g in range(pairs):
                dispatch_forward(s, g, oc).wait_recv()

        def gate_up(j, _):
            acc = jnp.dot(rows[s], wgu[j], preferred_element_type=f32)
            part, up = acc[:, :LANES], acc[:, LANES:]
            value = part / (1.0 + jnp.exp(-part)) * up
            hidden[:, pl.ds(pl.multiple_of(j * LANES, LANES), LANES)] = value.astype(bf16)
            return 0

        lax.fori_loop(0, blocks_f, gate_up, 0, unroll=True)
        tile = min(256, pw)

        def down(dst, side, h):
            for j in range(pw // tile):
                start = pl.multiple_of(side * hw + h * pw + j * tile, LANES)
                acc = jnp.dot(hidden[...], wd[:, pl.ds(start, tile)], preferred_element_type=f32)
                dst[s, :, h * pw + j * tile : h * pw + (j + 1) * tile] = acc.astype(bf16)

        if s == 0:
            loads["wd"].wait()
        for h in range(pieces):
            down(pair_out, oc, h)
            pair_copy(s, h).start()
        for h in range(pieces):
            down(psum, c, h)

    far = (1 - z // 2) * 2

    def end_copy(s, h):
        return remote(
            psum.at[s, zrows(far, 2), piece(h)], from_end.at[s, :, piece(h)],
            end_send.at[s, h], end_recv.at[s, h], mate_dev,
        )

    def mate_copy(s, h):
        return remote(
            psum.at[s, zrows(mate), piece(h)], from_mate.at[s, :, piece(h)],
            mate_send.at[s, h], mate_recv.at[s, h], mate_dev,
        )

    def inner_copy(s, h):
        return remote(
            psum.at[s, zrows(far, 2), piece(h)], from_inner.at[s, :, piece(h)],
            inner_send.at[s, h], inner_recv.at[s, h], across_dev,
        )

    def add_into(s, at, h, other):
        psum[s, at, piece(h)] = (psum[s, at, piece(h)].astype(f32) + other.astype(f32)).astype(bf16)

    def stage1(s):
        for h in range(pieces):
            pair_copy(s, h).wait_recv()

            def body(k, _):
                at = zrows(k)
                add_into(s, at, h, pair_in[s, at, piece(h)])
                return 0

            lax.fori_loop(0, pairs, body, 0)

            @pl.when(is_end)
            def _():
                end_copy(s, h).start()

    def stage2(s, h):
        end_copy(s, h).wait_recv()

        def body(k, _):
            add_into(s, zrows(far + k), h, from_end[s, zrows(k), piece(h)])
            return 0

        lax.fori_loop(0, 2, body, 0)
        inner_copy(s, h).start()

    def stage3(s, h):
        inner_copy(s, h).wait_recv()
        add_into(s, zrows(mate), h, from_inner[s, zrows(mate % 2), piece(h)])
        mate_copy(s, h).start()

    def inner(work):
        def run():
            @pl.when(is_inner)
            def _():
                work()

        return run

    def result_copy(s, h):
        return remote(
            result_out.at[s, :, piece(h)], results.at[pl.ds(s * cp, cp), piece(h)],
            ret_send.at[s - 1, h], ret_recv.at[s - 1, h], ep_peer[s],
        )

    def stage4(s, h, inside):
        mate_copy(s, h).wait_recv()
        total = psum[s, zrows(z), piece(h)].astype(f32) + from_mate[s, :, piece(h)].astype(f32)
        if inside:
            total = total + from_inner[s, zrows(z % 2), piece(h)].astype(f32)
        if s:
            result_out[s, :, piece(h)] = total.astype(bf16)
            result_copy(s, h).start()
        else:
            results[0:cp, piece(h)] = total.astype(bf16)

    def carry_copy(s):
        return remote(carries.at[0], carries.at[s], carry_send.at[s - 1], carry_recv.at[s - 1], ep_peer[s])

    def recurrence(services):
        state[...] = jnp.zeros_like(state)
        base[...] = jnp.zeros_like(base)
        n = CHUNK
        at = lax.broadcasted_iota(jnp.int32, (n, n), 0)
        of = lax.broadcasted_iota(jnp.int32, (n, n), 1)
        same = (at >= of) & (at // BLOCK_POSITIONS == of // BLOCK_POSITIONS)
        lower = jnp.where(same, 1.0, 0.0).astype(bf16)
        er = lax.broadcasted_iota(jnp.int32, (8, n), 0)
        pick_row = lax.broadcasted_iota(jnp.int32, (8, keys), 0)
        pick_head = lax.broadcasted_iota(jnp.int32, (8, keys), 1) // KEY_DIM
        pick = jnp.where((pick_row % heads == pick_head) & (pick_row < 3 * heads), 1.0, 0.0).astype(bf16)
        small = (BLOCK_POSITIONS, BLOCK_POSITIONS)
        causal = lax.broadcasted_iota(jnp.int32, small, 0) >= lax.broadcasted_iota(jnp.int32, small, 1)
        lane_head = lax.broadcasted_iota(jnp.int32, (BLOCK_POSITIONS, vals), 1) // VAL_DIM

        def chunk(i, _):
            for when, work in services.items():

                @pl.when(i == when)
                def _():
                    work()

            start = pl.multiple_of(i * n, n)
            here = pl.ds(start, n)
            qc = q[here, :].astype(f32)
            qc = qc / (1.0 + jnp.exp(-qc))
            key = gap_ref[...] / (1.0 + jnp.exp(f[here, :].astype(f32)))
            terms = jnp.zeros((8, n), f32)
            for h in range(heads):
                value = jnp.broadcast_to(extra_ref[h : h + 1, here], (8, n))
                one = value.astype(bf16).astype(f32)
                second = (value - one).astype(bf16).astype(f32)
                third = value - one - second
                terms = jnp.where(er == h, one, terms)
                terms = jnp.where(er == heads + h, second, terms)
                terms = jnp.where(er == 2 * heads + h, third, terms)
            extra = lax.dot_general(terms.astype(bf16), pick, TN, preferred_element_type=f32)
            log_forget = jnp.log(1.0 - key) + extra
            high = log_forget.astype(bf16)
            low = (log_forget - high.astype(f32)).astype(bf16)
            cumulative = jnp.dot(lower, high, preferred_element_type=f32) + jnp.dot(
                lower, low, preferred_element_type=f32
            )
            held = [state[h] for h in range(heads)]
            before = base[...]
            mid_at = BLOCK_POSITIONS // 2
            for b in range(n // BLOCK_POSITIONS):
                part = slice(b * BLOCK_POSITIONS, (b + 1) * BLOCK_POSITIONS)
                block = pl.ds(start + b * BLOCK_POSITIONS, BLOCK_POSITIONS)
                cum = cumulative[part]
                mid, last = cum[mid_at - 1 : mid_at], cum[BLOCK_POSITIONS - 1 :]
                q_part = qc[part]
                q_mid = (q_part * jnp.exp(cum - mid)).astype(bf16)
                k_mid = (key[part] * jnp.exp(mid - cum)).astype(bf16)
                qdec[block, :] = (q_part * jnp.exp(cum + before)).astype(bf16)
                decay_mid, decay_last, decay_rest = jnp.exp(mid), jnp.exp(last), jnp.exp(last - mid)
                before = before + last
                values = v[block, :]
                out = jnp.zeros((BLOCK_POSITIONS, vals), f32)
                for h in range(heads):
                    lanes = slice(h * KEY_DIM, (h + 1) * KEY_DIM)
                    across = lax.dot_general(
                        q_mid[:, lanes],
                        (held[h] * decay_mid[:, lanes]).astype(bf16),
                        NT,
                        preferred_element_type=f32,
                    )
                    scores = lax.dot_general(q_mid[:, lanes], k_mid[:, lanes], NT, preferred_element_type=f32)
                    scores = jnp.where(causal, scores, 0.0).astype(bf16)
                    within = jnp.dot(scores, values, preferred_element_type=f32)
                    out = jnp.where(lane_head == h, within + across, out)
                    update = lax.dot_general(values, k_mid[:, lanes], TN, preferred_element_type=f32)
                    held[h] = held[h] * decay_last[:, lanes] + update * decay_rest[:, lanes]
                rec[block, :] = out
            for h in range(heads):
                state[h] = held[h]
            base[...] = before
            return 0

        lax.fori_loop(0, length // n, chunk, 0)
        own = [state[h, h * VAL_DIM : (h + 1) * VAL_DIM, :] for h in range(heads)]
        carries[0, :VAL_DIM, :] = jnp.concatenate(own, axis=1).astype(bf16)
        total = jnp.exp(base[...])
        carries[0, VAL_DIM:, :] = jnp.broadcast_to(total, (16, keys)).astype(bf16)
        for s in range(1, places):
            carry_copy(s).start()

    chunk_rows = length // ROW_CHUNKS

    def rows_of(r):
        return pl.ds(r * chunk_rows, chunk_rows)

    def own_copy(r, side):
        here = mixed_all.at[z, side, rows_of(r)]
        return remote(here, here, own_send.at[r], own_recv.at[r], partner)

    def hop_right(src, r):
        here = mixed_all.at[src, c, rows_of(r)]
        to = {"tp": jnp.minimum(z + 1, last_z) * 2 + c}
        return remote(here, here, right_send.at[src, r], ag_recv.at[src, r], to)

    def hop_left(src, r):
        here = mixed_all.at[src, c, rows_of(r)]
        to = {"tp": jnp.maximum(z - 1, 0) * 2 + c}
        return remote(here, here, left_send.at[src, r], ag_recv.at[src, r], to)

    def ag_forward(src, r, side):
        here = mixed_all.at[src, side, rows_of(r)]
        return remote(here, here, agf_send.at[src, r], agf_recv.at[src, r], partner)

    def source(j, inside):
        at = (None, 2, 0, 3)[j] if inside else j
        return jnp.where(z < 2, at, last_z - at)

    def start_own(r):
        @pl.when(z < last_z)
        def _():
            hop_right(z, r).start()

        @pl.when(z > 0)
        def _():
            hop_left(z, r).start()

    def ag_step(j, inside, r):
        src = source(j, inside)
        hop_right(src, r).wait_recv()
        if inside:

            @pl.when(src < z)
            def _():
                hop_right(src, r).start()

            @pl.when(src > z)
            def _():
                hop_left(src, r).start()

        ag_forward(src, r, c).start()

    def gated():
        for s in range(1, places):
            carry_copy(s).wait_recv()
        total = jnp.zeros((VAL_DIM, keys), f32)
        for i in range(places):
            decay = carries[ep ^ i, VAL_DIM:, :].astype(f32)[:1]
            joined = total * decay + carries[ep ^ i, :VAL_DIM, :].astype(f32)
            total = jnp.where(i < ep, joined, total)
        lane_head = lax.broadcasted_iota(jnp.int32, total.shape, 1) // KEY_DIM
        for h in range(heads):
            held_state[h * VAL_DIM : (h + 1) * VAL_DIM, :] = jnp.where(lane_head == h, total, 0.0).astype(bf16)
        at = lax.broadcasted_iota(jnp.int32, (vals, vals), 0) // VAL_DIM
        of = lax.broadcasted_iota(jnp.int32, (vals, vals), 1) // VAL_DIM
        average = jnp.where(at == of, 1.0 / VAL_DIM, 0.0).astype(bf16)
        for r in range(ROW_CHUNKS):
            here = rows_of(r)
            whole = rec[here, :] + lax.dot_general(
                qdec[here, :], held_state[...], NT, preferred_element_type=f32
            )
            square = whole * whole
            high = square.astype(bf16)
            low = (square - high.astype(f32)).astype(bf16)
            mean = jnp.dot(high, average, preferred_element_type=f32) + jnp.dot(
                low, average, preferred_element_type=f32
            )
            opened = gate[here, :].astype(f32)
            opened = opened / (1.0 + jnp.exp(-opened))
            mixed = (whole * lax.rsqrt(mean + epsilon) * head_gain_ref[...] * opened).astype(bf16)
            mixed_all[z, c, here, :] = mixed

            @pl.when(is_inner)
            def _():
                start_own(r)

            own_copy(r, c).start()

    def out_copy(r):
        return pltpu.make_async_copy(out_buf.at[rows_of(r)], out_ref.at[rows_of(r)], out_sem.at[r])

    def moe_copy():
        return pltpu.make_async_copy(moe_buf, moe_ref, out_sem.at[ROW_CHUNKS])

    def project(j, inside, r):
        src = source(j, inside) if j else z
        if j:
            ag_forward(src, r, oc).wait_recv()
        else:
            own_copy(r, oc).wait_recv()
        here = rows_of(r)
        weight = wo[pl.ds(pl.multiple_of(src * 2 * vc, LANES), 2 * vc), :]
        both = jnp.concatenate([mixed_all[src, 0, here, :], mixed_all[src, 1, here, :]], axis=1)
        part = jnp.dot(both, weight, preferred_element_type=f32)
        if j:
            part = part + out_acc[here, :]
        if j == last_z:
            out_buf[here, :] = part.astype(bf16)
            out_copy(r).start()
        else:
            out_acc[here, :] = part

    def swap_copy():
        return remote(
            combined.at[pl.ds(pl.multiple_of(oc * sub, 16), sub)],
            moe_buf.at[:, half(c)], swap_send.at[0], swap_recv.at[0], partner,
        )

    def swap_in():
        return remote(
            combined.at[pl.ds(pl.multiple_of(oc * sub, 16), sub)],
            moe_buf.at[:, half(oc)], swap_send.at[0], swap_recv.at[0], partner,
        )

    def combine():
        lanes = pl.ds(pl.multiple_of(z * two, LANES), two)
        where_to, first, second = targets(lanes)
        weight = jnp.where(first, jnp.broadcast_to(weight_ref[0:1, lanes], (8, two)), 0.0) + jnp.where(
            second, jnp.broadcast_to(weight_ref[1:2, lanes], (8, two)), 0.0
        )
        high = weight.astype(bf16).astype(f32)
        low = weight - high
        picks = [slot_row == where_to[s : s + 1, :] for s in range(places)]
        coarse = jnp.concatenate(
            [jnp.where(picks[s], high[s : s + 1, :], 0.0).astype(bf16) for s in range(places)], axis=0
        )
        fine = jnp.concatenate(
            [jnp.where(picks[s], low[s : s + 1, :], 0.0).astype(bf16) for s in range(places)], axis=0
        )
        for s in range(1, places):
            for h in range(pieces):
                result_copy(s, h).wait_recv()
        total = lax.dot_general(coarse, results[...], TN, preferred_element_type=f32) + lax.dot_general(
            fine, results[...], TN, preferred_element_type=f32
        )
        combined[...] = total.astype(bf16)
        swap_copy().start()

    def finish():
        moe_buf[:, half(c)] = combined[pl.ds(pl.multiple_of(c * sub, 16), sub), :]
        swap_in().wait_recv()
        moe_copy().start()

    chunks = range(ROW_CHUNKS)
    both = range(pieces)
    for j in range(blocks_f):
        loads[("wg", j)].wait()
        loads[("wu", j)].wait()
    moe(0)
    for name in ("q", "f", "v", "gap", "extra"):
        loads[name].wait()

    def take(s, at):
        for g in at:
            forward(s, g)

    def second(s):
        for h in both:
            stage2(s, h)

    def third(s):
        for h in both:
            stage3(s, h)

    def mates(s):
        @pl.when(is_end)
        def _():
            for h in both:
                mate_copy(s, h).start()

    def starts(at):
        @pl.when(is_end)
        def _():
            for r in at:
                start_own(r)

    recurrence(
        {
            1: lambda: (stage1(0), mates(0)),
            3: lambda: (take(1, [0]), take(2, [0])),
            5: lambda: (take(1, [1]), take(2, [1])),
            6: inner(lambda: stage2(0, 0)),
            7: lambda: (take(1, [2]), take(2, [2])),
        }
    )
    take(1, [3])
    take(2, [3])
    inner(lambda: stage2(0, 1))()
    moe(1)
    stage1(1)
    moe(2)
    loads["gate"].wait()
    loads["head_gain"].wait()
    gated()
    inner(lambda: third(0))()
    stage1(2)
    take(3, range(pairs))
    moe(3)
    loads["wo"].wait()
    loads["weight"].wait()
    stage1(3)

    @pl.when(is_end)
    def _():
        for r in chunks:
            start_own(r)
        for s in range(1, places):
            for h in both:
                mate_copy(s, h).start()
        for r in chunks:
            project(0, False, r)
            ag_step(1, False, r)
        for h in both:
            stage4(0, h, False)
        for r in chunks:
            ag_step(2, False, r)
            project(1, False, r)
        for s in (1, 2):
            for h in both:
                stage4(s, h, False)
        for r in chunks:
            project(2, False, r)
        for r in (0, 1):
            ag_step(3, False, r)
        for h in both:
            stage4(3, h, False)
        for r in (2, 3):
            ag_step(3, False, r)
        for r in chunks:
            project(3, False, r)

    @pl.when(is_inner)
    def _():
        second(1)
        for r in chunks:
            project(0, True, r)
            ag_step(1, True, r)
        stage2(2, 0)
        stage3(1, 0)
        stage2(2, 1)
        stage3(1, 1)
        for r in chunks:
            project(1, True, r)
        stage2(3, 0)
        stage3(2, 0)
        stage2(3, 1)
        ag_step(2, True, 0)
        stage3(2, 1)
        ag_step(2, True, 1)
        ag_step(3, True, 0)
        stage3(3, 0)
        ag_step(2, True, 2)
        ag_step(3, True, 1)
        stage3(3, 1)
        ag_step(2, True, 3)
        ag_step(3, True, 2)
        ag_step(3, True, 3)
        for r in chunks:
            project(2, True, r)
        for s in range(places):
            for h in both:
                stage4(s, h, True)
        for r in chunks:
            project(3, True, r)

    combine()
    finish()

    for s in range(1, places):
        for g in range(pairs):
            dispatch(s, g).wait_send()
            dispatch_forward(s, g, c).wait_send()
        carry_copy(s).wait_send()
        for h in both:
            result_copy(s, h).wait_send()
    for s in range(places):
        for h in both:
            pair_copy(s, h).wait_send()
            mate_copy(s, h).wait_send()

            @pl.when(is_end)
            def _():
                end_copy(s, h).wait_send()

            @pl.when(is_inner)
            def _():
                inner_copy(s, h).wait_send()

    for r in chunks:
        own_copy(r, c).wait_send()
        out_copy(r).wait()
        for src in range(pairs):

            @pl.when((src <= z) & (z < last_z))
            def _():
                hop_right(src, r).wait_send()

            @pl.when((src >= z) & (z > 0))
            def _():
                hop_left(src, r).wait_send()

            @pl.when(src != z)
            def _():
                ag_forward(src, r, c).wait_send()

    swap_copy().wait_send()
    moe_copy().wait()


def on_device(*arrays):
    (
        query, forget, values, gate, gap, extra, head_gain, out_weight,
        tokens, norm_gain, index, weight, gate_weight, up_weight, down_weight,
    ) = arrays
    places, groups = lax.axis_size("ep"), lax.axis_size("tp")
    pairs = groups // 2
    length, keys = query.shape
    vals = values.shape[1]
    count, width = tokens.shape
    hidden = gate_weight.shape[2]
    sub = count // groups
    experts_all = gate_weight.shape[0] * places
    capacity = max(2, sub * TOPK * 5 // (4 * experts_all))
    fits = (
        places == 4
        and groups == 8
        and gate_weight.shape[0] == 1
        and 2 * sub == LANES
        and capacity % 8 == 0
        and capacity <= sub
        and vals == LANES
        and keys == 2 * KEY_DIM
        and length % (ROW_CHUNKS * CHUNK) == 0
        and hidden % LANES == 0
        and width % 512 == 0
    )
    if not fits:
        return general(*arrays)
    heads = keys // KEY_DIM
    cp = 2 * capacity
    rows_all = pairs * cp
    hw = width // 2
    features = out_weight.shape[1]
    bf16, f32 = jnp.bfloat16, jnp.float32
    vmem = pl.BlockSpec(memory_space=pltpu.VMEM)
    anywhere = pl.BlockSpec(memory_space=pl.ANY)
    dma = pltpu.SemaphoreType.DMA
    small = [index.T, weight.T, norm_gain.reshape(1, width), gap.reshape(1, keys), extra.T, head_gain.reshape(1, vals)]
    scratch = [pltpu.VMEM(a.shape, a.dtype) for a in small]
    scratch += [
        pltpu.VMEM((count, width), bf16),
        pltpu.VMEM((length, keys), bf16),
        pltpu.VMEM((length, keys), bf16),
        pltpu.VMEM((length, vals), bf16),
        pltpu.VMEM((length, vals), bf16),
        pltpu.VMEM(out_weight.shape, bf16),
        pltpu.VMEM((hidden // LANES, width, 2 * LANES), bf16),
        pltpu.VMEM((hidden, width), bf16),
        pltpu.VMEM((places - 1, rows_all, hw), bf16),
        pltpu.VMEM((places, rows_all, width), bf16),
        pltpu.VMEM((rows_all, hidden), bf16),
        pltpu.VMEM((places, rows_all, hw), bf16),
        pltpu.VMEM((places, rows_all, hw), bf16),
        pltpu.VMEM((places, rows_all, hw), bf16),
        pltpu.VMEM((places, 2 * cp, hw), bf16),
        pltpu.VMEM((places, cp, hw), bf16),
        pltpu.VMEM((places, 2 * cp, hw), bf16),
        pltpu.VMEM((places, cp, hw), bf16),
        pltpu.VMEM((places * cp, hw), bf16),
        pltpu.VMEM((2 * sub, hw), bf16),
        pltpu.VMEM((sub, width), bf16),
        pltpu.VMEM((heads, vals, KEY_DIM), f32),
        pltpu.VMEM((1, keys), f32),
        pltpu.VMEM((places, VAL_DIM + 16, keys), bf16),
        pltpu.VMEM((length, vals), f32),
        pltpu.VMEM((length, keys), bf16),
        pltpu.VMEM((vals, keys), bf16),
        pltpu.VMEM((pairs, 2, length, vals), bf16),
        pltpu.VMEM((length, features), f32),
        pltpu.VMEM((length, features), bf16),
    ]
    n_loads = pairs + 2 * (hidden // LANES) + 12
    peers = places - 1
    sems = [dma((n_loads,))]
    sems += [dma((peers, pairs))] * 4 + [dma((places, 2))] * 8 + [dma((peers, 2))] * 2 + [dma((1,))] * 2
    sems += [dma((peers,))] * 2 + [dma((ROW_CHUNKS,))] * 2 + [dma((pairs, ROW_CHUNKS))] * 5 + [dma((ROW_CHUNKS + 1,))]
    outputs = pl.pallas_call(
        fused_kernel,
        in_specs=[anywhere] * 15,
        out_specs=[anywhere, anywhere],
        out_shape=[
            jax.ShapeDtypeStruct((length, features), bf16),
            jax.ShapeDtypeStruct((sub, width), bf16),
        ],
        scratch_shapes=scratch + sems,
        compiler_params=pltpu.CompilerParams(
            collective_id=0, has_side_effects=True, vmem_limit_bytes=64 * 1024 * 1024 - 65536
        ),
        name="fused_layer",
    )(
        *small, tokens, query, forget, values, gate, out_weight,
        gate_weight, up_weight, down_weight,
    )
    parts = [(0, r * length // 4, length // 4) for r in range(4)] + [(1, 0, sub)]

    def deliver(first, second, out_first, out_second, buf, small_buf, sem_in, sem_out):
        sources, targets, bufs = (first, second), (out_first, out_second), (buf, small_buf)
        into = [
            pltpu.make_async_copy(sources[w].at[pl.ds(a, n)], bufs[w].at[pl.ds(a, n)], sem_in.at[i])
            for i, (w, a, n) in enumerate(parts)
        ]
        outof = [
            pltpu.make_async_copy(bufs[w].at[pl.ds(a, n)], targets[w].at[pl.ds(a, n)], sem_out.at[i])
            for i, (w, a, n) in enumerate(parts)
        ]
        for copy in into:
            copy.start()
        for i, copy in enumerate(into):
            copy.wait()
            outof[i].start()
        for copy in outof:
            copy.wait()

    return tuple(
        pl.pallas_call(
            deliver,
            in_specs=[anywhere] * 2,
            out_specs=[anywhere] * 2,
            out_shape=[jax.ShapeDtypeStruct((length, features), bf16), jax.ShapeDtypeStruct((sub, width), bf16)],
            scratch_shapes=[
                pltpu.VMEM((length, features), bf16),
                pltpu.VMEM((sub, width), bf16),
                dma((len(parts),)),
                dma((len(parts),)),
            ],
            name="deliver",
        )(*outputs)
    )


def solution(mesh):
    placed = (
        P("ep", "tp"),
        P("ep", "tp"),
        P("ep", "tp"),
        P("ep", "tp"),
        P("tp"),
        P("ep", "tp"),
        P("tp"),
        P(None, "tp"),
        P("ep", None),
        P(),
        P("ep", None),
        P("ep", None),
        P("ep", None, "tp"),
        P("ep", None, "tp"),
        P("ep", "tp", None),
    )
    return jax.shard_map(
        on_device,
        mesh=mesh,
        in_specs=placed,
        out_specs=(P("ep", "tp"), P(("ep", "tp"), None)),
        check_vma=False,
    )
```
